32 devices in a mesh: sp: 4 (over z), tp: 4 (over y, x), dp: 2 (over core).
Axes of the slice: x: 2, y: 2, z: 4, core: 2. Of those that a mesh axis runs over, the one named last changes fastest.
Arguments:
- latent: bfloat16 [2, 512, 2048], P('dp', ('sp', 'tp')), may hold values from -10 to 10
- condition: bfloat16 [2, 2048], P('dp'), may hold values from -6 to 6
- context: bfloat16 [2, 512, 2048], P('dp', 'sp'), may hold values from -6 to 6
- context_source: bfloat16 [2048], replicated, may hold values from -6 to 6
- mod_weight: bfloat16 [3, 2048, 2048], P(None, 'sp', 'tp'), may hold values from -0.125 to 0.125
- norm_gain: bfloat16 [2048], replicated, may hold values from 0.099609375 to 1.8984375
- w_x: bfloat16 [2048, 2048], P('dp', 'tp'), may hold values from -0.125 to 0.125
- w_b: bfloat16 [2048, 512], P('dp', 'tp'), may hold values from -0.125 to 0.125
- w_c: bfloat16 [2048, 512], P('dp', 'tp'), may hold values from -0.125 to 0.125
- w_z: bfloat16 [2048, 2048], P('dp', 'tp'), may hold values from -0.125 to 0.125
- w_dt: bfloat16 [2, 2048, 32], P(None, 'dp', 'tp'), may hold values from -0.125 to 0.125
- conv_x: bfloat16 [3, 2048], P(None, 'tp'), may hold values from -3.5 to 3.5
- conv_b: bfloat16 [3, 512], P(None, 'tp'), may hold values from -3.5 to 3.5
- conv_c: bfloat16 [3, 512], P(None, 'tp'), may hold values from -3.5 to 3.5
- decay_rate: float32 [2, 32], P(None, 'tp'), may hold values from 0 to 1, as said below
- out_gain: bfloat16 [2048], P('tp'), may hold values from 0.099609375 to 1.8984375
- w_out: bfloat16 [2048, 2048], P(('tp', 'dp')), may hold values from -0.125 to 0.125
Outputs:
- update: bfloat16 [2, 512, 2048], P('dp', ('sp', 'tp'))
The draws below stay inside these ranges and needn't reach their ends.
Inputs may be any that keep to these rules, and one draw needn't show every extreme that they name: `decay_rate`: positive rates.
All inputs are finite; a program needn't handle non-finite values.
Results may differ from the reference program's by a relative error of at most 0.014.
Values may be sent and summed in bfloat16 or wider, within the bound.
A program may use at most 128 MiB of HBM per device.

```python
import jax
import jax.numpy as jnp
from jax import lax

D = 2048
HEADS = 32
HEAD_DIM = 64
GROUPS = 4
STATE = 128
CONV = 3
BLOCK = 128
TOK_DEV = 128
CTX = 512
INNER = 2048
SEQ = 512
BATCH = 2
N_TP = 4


def draw_latent(key, part):
    noise_key, dir_key, span_key, block_key = jax.random.split(key, 4)
    shape = (BATCH, SEQ, D)
    noise = jax.random.truncated_normal(noise_key, -4.0, 4.0, shape, jnp.float32)
    direction = jax.random.truncated_normal(dir_key, -3.0, 3.0, (D,), jnp.float32)
    coarse = jnp.repeat(jax.random.uniform(span_key, (BATCH, SEQ // TOK_DEV, 1), jnp.float32, -1.5, 1.5), TOK_DEV, axis=1)
    finer = jnp.repeat(jax.random.uniform(block_key, (BATCH, SEQ // BLOCK, 1), jnp.float32, -0.5, 0.5), BLOCK, axis=1)
    return (noise + (coarse + finer) * direction).astype(jnp.bfloat16)


def draw_decay_rate(key, part):
    slow_key, fast_key, pick_key = jax.random.split(key, 3)
    chain = SEQ + CTX
    slow_rate = jax.random.uniform(slow_key, (2, HEADS), jnp.float32, 0.6, 2.0) / chain
    fast_rate = jax.random.uniform(fast_key, (2, HEADS), jnp.float32, 0.015, 0.04)
    picked = jax.random.uniform(pick_key, (2, HEADS), jnp.float32) < 0.25
    return jnp.where(picked, fast_rate, slow_rate)


def levels(rng, shape, cuts, smallest, top_value):
    def one(axis_at, blocks):
        steps = jax.random.uniform(jax.random.fold_in(jax.random.fold_in(rng, 6), axis_at), (blocks,), jnp.float32, smallest / len(cuts), top_value / len(cuts))
        return jnp.repeat(jnp.exp(steps), shape[axis_at] // blocks).reshape((-1,) + (1,) * (len(shape) - axis_at - 1))

    loudness = one(*cuts[0])
    for cut in cuts[1:]:
        loudness = loudness * one(*cut)
    return loudness


def gaussian(rng, shape, scale, limit, cuts=(), held_as=jnp.bfloat16):
    values = jax.random.normal(rng, shape, jnp.float32) * scale
    if len(cuts) > 0:
        values = levels(rng, shape, cuts, -0.22, 0.18) * values
    return jnp.clip(values, min=-limit, max=limit).astype(held_as)


def setup_inputs(seed: int = 0) -> dict:
    key_of = jax.random.split(jax.random.key(seed), 18)
    latent = draw_latent(jax.random.fold_in(key_of[17], 71), 0)
    condition = gaussian(key_of[1], (BATCH, D), 1.0, 6.0, ((0, 2),))
    context = gaussian(key_of[2], (BATCH, CTX, D), 1.0, 6.0, ((0, 2), (1, 4)))
    context_source = gaussian(key_of[3], (D,), 1.0, 6.0)
    mod_weight = gaussian(key_of[4], (3, D, D), D ** -0.5, 0.125, ((1, 4), (2, 4)))
    norm_gain = jnp.clip(1.0 + 0.18 * jax.random.normal(key_of[5], (D,), jnp.float32), 0.099609375, 1.8984375).astype(jnp.bfloat16)
    w_x = gaussian(key_of[6], (D, INNER), D ** -0.5, 0.125, ((0, 2), (1, 4)))
    w_b = gaussian(key_of[7], (D, GROUPS * STATE), D ** -0.5, 0.125, ((0, 2), (1, 4)))
    w_c = gaussian(key_of[8], (D, GROUPS * STATE), D ** -0.5, 0.125, ((0, 2), (1, 4)))
    w_z = gaussian(key_of[9], (D, INNER), D ** -0.5, 0.125, ((0, 2), (1, 4)))
    w_dt = gaussian(key_of[10], (2, D, HEADS), D ** -0.5, 0.125, ((1, 2), (2, 4)))
    conv_x = gaussian(key_of[11], (CONV, INNER), CONV ** -0.5, 3.5, ((1, 4),))
    conv_b = gaussian(key_of[12], (CONV, GROUPS * STATE), CONV ** -0.5, 3.5, ((1, 4),))
    conv_c = gaussian(key_of[13], (CONV, GROUPS * STATE), CONV ** -0.5, 3.5, ((1, 4),))
    decay_rate = draw_decay_rate(jax.random.fold_in(key_of[17], 71), 0)
    out_gain = jnp.clip(1.0 + 0.18 * jax.random.normal(key_of[15], (INNER,), jnp.float32), 0.099609375, 1.8984375).astype(jnp.bfloat16)
    w_out = gaussian(key_of[16], (INNER, D), INNER ** -0.5, 0.125, ((0, 8),))
    return dict(latent=latent, condition=condition, context=context, context_source=context_source, mod_weight=mod_weight, norm_gain=norm_gain, w_x=w_x, w_b=w_b, w_c=w_c, w_z=w_z, w_dt=w_dt, conv_x=conv_x, conv_b=conv_b, conv_c=conv_c, decay_rate=decay_rate, out_gain=out_gain, w_out=w_out)


EPSILON = 1e-06

def rounded(values):
    return lax.optimization_barrier(values.astype(jnp.bfloat16)).astype(jnp.float32)

def modulated(source, gain_vec, shift_vec, scale_vec):
    values = source.astype(jnp.float32)
    normed = values * lax.rsqrt(lax.optimization_barrier(jnp.mean(values * values, axis=-1, keepdims=True)) + EPSILON)
    return (normed * gain_vec.astype(jnp.float32) * (1.0 + scale_vec) + shift_vec).astype(jnp.bfloat16)

def project(source, weight):
    return jnp.dot(source, weight, preferred_element_type=jnp.float32).astype(jnp.bfloat16)

def centred_conv(source, weight):
    total_rows = source.shape[0]
    reach_rows = weight.shape[0] // 2
    padded = jnp.pad(source.astype(jnp.float32), ((reach_rows, reach_rows), (0, 0)))
    tap_weights = weight.astype(jnp.float32)
    summed = jnp.zeros(source.shape, jnp.float32)
    for offset in range(weight.shape[0]):
        summed = summed + padded[offset:offset + total_rows] * tap_weights[offset]
    return jax.nn.silu(summed).astype(jnp.bfloat16)

def final_state(x_vals, b_vals, step_size, rate_head):
    total_rows, head_count = step_size.shape
    per_group = head_count // GROUPS
    moved_x = rounded(x_vals.reshape(total_rows, head_count, HEAD_DIM).astype(jnp.float32) * step_size[:, :, None])
    running = jnp.cumsum(-rate_head * step_size, axis=0)
    weight = jnp.exp(running[-1:] - running)
    scaled = (moved_x * weight[:, :, None]).reshape(total_rows, GROUPS, per_group, HEAD_DIM)
    b_wide = b_vals.reshape(total_rows, GROUPS, STATE).astype(jnp.float32)
    return jnp.einsum('sgn,sghp->ghpn', b_wide, scaled, precision=lax.Precision.HIGHEST)

def ssd_direction(x_vals, b_vals, c_vals, step_size, rate_head, start_state):
    total_rows, head_count = step_size.shape
    per_group = head_count // GROUPS
    blocks = total_rows // BLOCK
    moved_x = rounded(x_vals.reshape(total_rows, head_count, HEAD_DIM).astype(jnp.float32) * step_size[:, :, None])
    decay_log = -rate_head * step_size
    lower_part = jnp.arange(BLOCK)[:, None] >= jnp.arange(BLOCK)[None, :]

    def advance(carried_in, inputs):
        x_block, b_block, c_block, d_block = inputs
        running = jnp.cumsum(d_block, axis=0)
        across = running.T
        spread = across[:, :, None] - across[:, None, :]
        decay_mask = jnp.where(lower_part, jnp.exp(jnp.minimum(spread, 0.0)), 0.0).reshape(GROUPS, per_group, BLOCK, BLOCK)
        b_wide = b_block.astype(jnp.float32)
        c_wide = c_block.astype(jnp.float32)
        scores = jnp.einsum('lgn,sgn->gls', c_wide, b_wide)
        weights = rounded(scores[:, None] * decay_mask)
        x_group = x_block.reshape(BLOCK, GROUPS, per_group, HEAD_DIM)
        inside = jnp.einsum('ghls,sghp->lghp', weights, x_group)
        carried = jnp.einsum('lgn,ghpn->lghp', c_wide, rounded(carried_in))
        growth = jnp.exp(running).reshape(BLOCK, GROUPS, per_group, 1)
        to_end = jnp.exp(running[-1:] - running).reshape(BLOCK, GROUPS, per_group, 1)
        fresh_state = jnp.einsum('sgn,sghp->ghpn', b_wide, rounded(x_group * to_end))
        ending = carried_in * jnp.exp(running[-1]).reshape(GROUPS, per_group, 1, 1) + fresh_state
        return (ending, inside + growth * carried)
    _, outputs = lax.scan(advance, start_state, (moved_x.reshape(blocks, BLOCK, head_count, HEAD_DIM), b_vals.reshape(blocks, BLOCK, GROUPS, STATE), c_vals.reshape(blocks, BLOCK, GROUPS, STATE), decay_log.reshape(blocks, BLOCK, head_count)))
    return outputs.reshape(total_rows, head_count * HEAD_DIM)

def reference(latent, condition, context, context_source, mod_weight, norm_gain, w_x, w_b, w_c, w_z, w_dt, conv_x, conv_b, conv_c, decay_rate, out_gain, w_out):
    activation = rounded(jax.nn.silu(condition.astype(jnp.float32)))
    source_act = rounded(jax.nn.silu(context_source.astype(jnp.float32)))
    weight_wide = mod_weight.astype(jnp.float32)
    mod_latent = jnp.einsum('bd,kdc->kbc', activation, weight_wide)
    mod_context = jnp.einsum('d,kdc->kc', source_act, weight_wide)
    part_width = INNER // N_TP
    outputs = []
    for sample in range(latent.shape[0]):
        ctx_rows = modulated(context[sample], norm_gain, mod_context[0], mod_context[1])
        ctx_x = centred_conv(project(ctx_rows, w_x), conv_x)
        ctx_b = centred_conv(project(ctx_rows, w_b), conv_b)
        ctx_fwd = jax.nn.softplus(project(ctx_rows, w_dt[0]).astype(jnp.float32))
        ctx_bwd = jax.nn.softplus(project(ctx_rows, w_dt[1]).astype(jnp.float32))
        state_fwd = final_state(ctx_x, ctx_b, ctx_fwd, decay_rate[0])
        state_bwd = final_state(jnp.flip(ctx_x, 0), jnp.flip(ctx_b, 0), jnp.flip(ctx_bwd, 0), decay_rate[1])
        latent_rows = modulated(latent[sample], norm_gain, mod_latent[0, sample], mod_latent[1, sample])
        x_vals = centred_conv(project(latent_rows, w_x), conv_x)
        b_vals = centred_conv(project(latent_rows, w_b), conv_b)
        c_vals = centred_conv(project(latent_rows, w_c), conv_c)
        step_fwd = jax.nn.softplus(project(latent_rows, w_dt[0]).astype(jnp.float32))
        step_bwd = jax.nn.softplus(project(latent_rows, w_dt[1]).astype(jnp.float32))
        gate_in = project(latent_rows, w_z)
        total_rows = latent_rows.shape[0]
        out_fwd = ssd_direction(x_vals, b_vals, c_vals, step_fwd, decay_rate[0], state_fwd)
        out_bwd = jnp.flip(ssd_direction(jnp.flip(x_vals, 0), jnp.flip(b_vals, 0), jnp.flip(c_vals, 0), jnp.flip(step_bwd, 0), decay_rate[1], state_bwd), 0)
        gated = (out_fwd + out_bwd) * jax.nn.silu(gate_in.astype(jnp.float32))
        grouped = gated.reshape(total_rows, GROUPS, -1)
        normed = grouped * lax.rsqrt(lax.optimization_barrier(jnp.mean(grouped * grouped, axis=-1, keepdims=True)) + EPSILON) * out_gain.reshape(GROUPS, -1).astype(jnp.float32)
        normed_out = normed.reshape(total_rows, -1).astype(jnp.bfloat16)
        mixed = jnp.zeros((total_rows, w_out.shape[1]), jnp.float32)
        for part_idx in range(N_TP):
            lower_col = part_idx * part_width
            term = jnp.dot(normed_out[:, lower_col:lower_col + part_width], w_out[lower_col:lower_col + part_width], preferred_element_type=jnp.float32)
            mixed = mixed + rounded(term)
        outputs.append((mod_latent[2, sample] * mixed).astype(jnp.bfloat16))
    return jnp.stack(outputs)
```

```python
import functools

import jax
import jax.numpy as jnp
from jax import lax
from jax.experimental import pallas as pl
from jax.experimental.pallas import tpu as pltpu
from jax.sharding import PartitionSpec as P

STATE = 128
LANES = 128
PAD = 16
EPSILON = 1e-06
MESH = pl.DeviceIdType.MESH
F32 = jnp.float32
BF16 = jnp.bfloat16


def silu(v):
    return v / (1.0 + jnp.exp(-v))


def softplus(v):
    return jnp.maximum(v, 0.0) + jnp.log1p(jnp.exp(-jnp.abs(v)))


def dot(a, b, dims=((1,), (0,)), precision=None):
    return lax.dot_general(a, b, (dims, ((), ())), precision=precision, preferred_element_type=F32)


def kernel(
    n_sp,
    n_tp,
    n_dp,
    heads,
    acts,
    edges,
    gain,
    conv_x,
    conv_b,
    conv_c,
    rate,
    out_gain,
    latent,
    context,
    mod_weight,
    w_x,
    w_b,
    w_c,
    w_dt,
    w_z,
    w_out,
    out,
    lat_all,
    ctx_buf,
    mod_buf,
    wx,
    wb,
    wc,
    wd,
    wz,
    wo,
    part,
    part_all,
    mods,
    halo,
    hid,
    snd_a,
    rcv_a,
    tot,
    snd_b,
    rcv_b,
    snd_o,
    rcv_o,
    local_sem,
    dp_send,
    dp_recv,
    lat_send,
    lat_recv,
    mod1_send,
    mod1_recv,
    mod2_send,
    mod2_recv,
    edge_send,
    edge_recv,
    a_send,
    a_recv,
    t_send,
    t_recv,
    b_send,
    b_recv,
    o_send,
    o_recv,
):
    s = lax.axis_index("sp")
    t = lax.axis_index("tp")
    d = lax.axis_index("dp")
    own_rows, width = latent.shape
    ctx_rows = context.shape[0]
    rows = n_tp * own_rows
    inner = w_x.shape[1]
    both = 2 * inner
    head_dim = inner // heads
    nh2 = 2 * heads

    def remote(src, dst, send, recv, **to):
        return pltpu.make_async_remote_copy(
            src_ref=src, dst_ref=dst, send_sem=send, recv_sem=recv, device_id=to, device_id_type=MESH
        )

    local = []

    def fetch(src, dst):
        copy = pltpu.make_async_copy(src, dst, local_sem.at[len(local)])
        copy.start()
        local.append(copy)
        return copy

    mod_copy = fetch(mod_weight, mod_buf)
    lat_copy = fetch(latent, lat_all.at[t])
    ctx_copy = fetch(context, ctx_buf)
    lat_moves = []
    for k in range(1, n_tp):
        lat_moves.append(
            remote(latent, lat_all.at[t], lat_send.at[k], lat_recv.at[k], tp=lax.rem(t + k, n_tp))
        )
        lat_moves[-1].start()
    up, down = lax.rem(s + 1, n_sp), lax.rem(s + n_sp - 1, n_sp)
    ctx_up = remote(edges.at[3], halo.at[2], edge_send.at[0], edge_recv.at[2], sp=up)
    ctx_down = remote(edges.at[2], halo.at[3], edge_send.at[1], edge_recv.at[3], sp=down)
    ctx_up.start()
    ctx_down.start()
    lat_up = [
        remote(edges.at[1], halo.at[0], edge_send.at[2 + u], edge_recv.at[0], sp=up, tp=u)
        for u in range(n_tp)
    ]
    lat_down = [
        remote(edges.at[0], halo.at[1], edge_send.at[2 + n_tp + u], edge_recv.at[1], sp=down, tp=u)
        for u in range(n_tp)
    ]

    @pl.when(t == n_tp - 1)
    def _():
        for copy in lat_up:
            copy.start()

    @pl.when(t == 0)
    def _():
        for copy in lat_down:
            copy.start()

    weight_moves = []
    pairs = ((w_x, wx), (w_b, wb), (w_dt, wd), (w_c, wc), (w_z, wz), (w_out, wo))
    for i, (src, dst) in enumerate(pairs):
        depth = src.shape[0]
        place = dst.at[pl.ds(d * depth, depth)]
        for k in range(1, n_dp):
            at = i * n_dp + k
            weight_moves.append(
                remote(src, place, dp_send.at[at], dp_recv.at[at], dp=lax.rem(d + k, n_dp))
            )
            weight_moves[-1].start()
        fetch(src, place)

    mod_copy.wait()
    pieces = [dot(acts[...], mod_buf[k])[0:2] for k in range(mod_buf.shape[0])]
    cols = pieces[0].shape[1]
    part[...] = jnp.concatenate(pieces + [jnp.zeros((2, cols), F32)], axis=0)
    moves = []
    for k in range(1, n_sp):
        moves.append(
            remote(part, part_all.at[k], mod1_send.at[k], mod1_recv.at[k], sp=lax.rem(s + k, n_sp))
        )
        moves[-1].start()
    summed = part[...]
    for k in range(1, n_sp):
        moves[k - 1].wait()
        summed = summed + part_all[k]
    mods[t] = summed
    moves = []
    for k in range(1, n_tp):
        moves.append(
            remote(mods.at[t], mods.at[t], mod2_send.at[k], mod2_recv.at[k], tp=lax.rem(t + k, n_tp))
        )
        moves[-1].start()
    for copy in moves:
        copy.wait()

    def vector(row):
        return jnp.concatenate([mods[c][row : row + 1] for c in range(n_tp)], axis=1)

    def normed(v, gains, shift):
        return v * lax.rsqrt(jnp.mean(v * v, axis=1, keepdims=True) + EPSILON) * gains + shift

    gain_row = gain[...].astype(F32)
    lat_shift, ctx_shift = vector(0), vector(1)
    lat_gain = gain_row * (1.0 + vector(2))
    ctx_gain = gain_row * (1.0 + vector(3))
    ctx_copy.wait()
    step_rows = min(32, ctx_rows)
    for r in range(0, ctx_rows, step_rows):
        block = ctx_buf[r : r + step_rows].astype(F32)
        hid[rows + PAD + r : rows + PAD + r + step_rows] = normed(block, ctx_gain, ctx_shift).astype(BF16)
    lat_copy.wait()
    for copy in lat_moves:
        copy.wait()
    for u in range(n_tp):
        hid[u * own_rows : (u + 1) * own_rows] = normed(
            lat_all[u].astype(F32), lat_gain, lat_shift
        ).astype(BF16)
    ctx_up.wait_send()
    ctx_down.wait_send()
    ctx_up.wait_recv()
    ctx_down.wait_recv()
    lat_up[0].wait_recv()
    lat_down[0].wait_recv()

    @pl.when(t == n_tp - 1)
    def _():
        for copy in lat_up:
            copy.wait_send()

    @pl.when(t == 0)
    def _():
        for copy in lat_down:
            copy.wait_send()

    hid[rows : rows + PAD] = jnp.concatenate(
        [
            normed(halo[0], lat_gain, lat_shift),
            normed(halo[1], lat_gain, lat_shift),
            normed(halo[2], ctx_gain, ctx_shift),
            normed(halo[3], ctx_gain, ctx_shift),
            jnp.zeros((PAD - 4, width), F32),
        ],
        axis=0,
    ).astype(BF16)
    for copy in weight_moves:
        copy.wait()
    for copy in local[3:]:
        copy.wait()

    has_before = s > 0
    has_after = s < n_sp - 1

    def shaped(values, before, after, taps):
        count = values.shape[0]
        at = lax.broadcasted_iota(jnp.int32, values.shape, 0)
        before = jnp.where(has_before, before, 0.0)
        after = jnp.where(has_after, after, 0.0)
        earlier = jnp.where(at == 0, before, pltpu.roll(values, 1, 0))
        later = jnp.where(at == count - 1, after, pltpu.roll(values, count - 1, 0))
        w = taps[...].astype(F32)
        return silu(earlier * w[0:1] + values * w[1:2] + later * w[2:3]).astype(BF16)

    def project(weight, count):
        return dot(hid[0:count], weight[...]).astype(BF16).astype(F32)

    total = rows + PAD + ctx_rows
    px = project(wx, total)
    x_in = shaped(px[0:rows], px[rows : rows + 1], px[rows + 1 : rows + 2], conv_x).astype(F32)
    cx_in = shaped(
        px[rows + PAD :], px[rows + 2 : rows + 3], px[rows + 3 : rows + 4], conv_x
    ).astype(F32)
    pb = project(wb, total)
    b_in = shaped(pb[0:rows], pb[rows : rows + 1], pb[rows + 1 : rows + 2], conv_b)
    cb_in = shaped(pb[rows + PAD :], pb[rows + 2 : rows + 3], pb[rows + 3 : rows + 4], conv_b)
    step_all = softplus(project(wd, total))

    spread_at = lax.broadcasted_iota(jnp.int32, (LANES, both), 0)
    spread_to = lax.broadcasted_iota(jnp.int32, (LANES, both), 1) // head_dim
    spreader = jnp.where((spread_to == spread_at) | (spread_to + nh2 == spread_at), 1.0, 0.0).astype(BF16)

    def expand(v):
        lane = lax.broadcasted_iota(jnp.int32, v.shape, 1)
        high = v.astype(BF16).astype(F32)
        low = pltpu.roll(v - high, nh2, 1)
        packed = jnp.where(lane < nh2, high, jnp.where(lane < 2 * nh2, low, 0.0))
        return dot(packed.astype(BF16), spreader)

    def running(steps):
        count = steps.shape[0]
        logs = -rate[...] * steps
        a = lax.broadcasted_iota(jnp.int32, (count, count), 0)
        b = lax.broadcasted_iota(jnp.int32, (count, count), 1)
        lower = jnp.where(a >= b, 1.0, 0.0)
        upper = jnp.where(a <= b, 1.0, 0.0)
        lane = lax.broadcasted_iota(jnp.int32, logs.shape, 1)
        sums = jnp.where(
            lane < heads,
            dot(lower, logs, precision=lax.Precision.HIGHEST),
            dot(upper, logs, precision=lax.Precision.HIGHEST),
        )
        row_lane = lax.broadcasted_iota(jnp.int32, (1, LANES), 1)
        ends = jnp.where(row_lane < heads, sums[count - 1 : count], sums[0:1])
        return sums, ends

    def moved(values, steps):
        wide = jnp.concatenate([values, values], axis=1)
        return (wide * expand(steps)).astype(BF16)

    c_steps = step_all[rows + PAD :]
    c_sums, c_ends = running(c_steps)
    c_moved = moved(cx_in, c_steps)
    c_scaled = (c_moved.astype(F32) * expand(jnp.exp(c_ends - c_sums))).astype(BF16)
    c_state = dot(cb_in, c_scaled, ((0,), (0,)))
    l_steps = step_all[0:rows]
    l_sums, l_ends = running(l_steps)
    l_moved = moved(x_in, l_steps)
    l_scaled = (l_moved.astype(F32) * expand(jnp.exp(l_ends - l_sums))).astype(BF16)
    l_state = dot(b_in, l_scaled, ((0,), (0,)))
    state_rows = STATE // n_sp
    for r in range(n_sp):
        cut = slice(r * state_rows, (r + 1) * state_rows)
        snd_a[r, :, 0:both] = c_state[cut].astype(BF16)
        snd_a[r, :, both : 2 * both] = l_state[cut].astype(BF16)
    ends = jnp.exp(jnp.concatenate([c_ends, l_ends, jnp.zeros((6, LANES), F32)], axis=0))
    tot[s] = expand(ends)
    a_moves, t_moves = [], []
    for k in range(1, n_sp):
        to = lax.rem(s + k, n_sp)
        a_moves.append(remote(snd_a.at[to], rcv_a.at[s], a_send.at[k], a_recv.at[k], sp=to))
        a_moves[-1].start()
        t_moves.append(remote(tot.at[s], tot.at[s], t_send.at[k], t_recv.at[k], sp=to))
        t_moves[-1].start()
    rcv_a[s] = snd_a[s]

    pc = project(wc, rows + PAD)
    c_in = shaped(pc[0:rows], pc[rows : rows + 1], pc[rows + 1 : rows + 2], conv_c)
    scores = dot(c_in, b_in, ((1,), (1,)))
    at_t = lax.broadcasted_iota(jnp.int32, (rows, rows), 0)
    at_s = lax.broadcasted_iota(jnp.int32, (rows, rows), 1)
    sums_t = jnp.transpose(l_sums)

    def weights(lane, keep):
        gap = l_sums[:, lane : lane + 1] - sums_t[lane : lane + 1]
        return jnp.where(keep, scores * jnp.exp(jnp.minimum(gap, 0.0)), 0.0).astype(BF16)

    pair = LANES // head_dim
    inside = []
    lane_head = lax.broadcasted_iota(jnp.int32, (rows, LANES), 1) // head_dim
    for p in range(heads // pair):
        cut = slice(p * LANES, (p + 1) * LANES)
        cut_b = slice(inner + p * LANES, inner + (p + 1) * LANES)
        source = jnp.concatenate([l_moved[:, cut], l_moved[:, cut_b]], axis=0)
        value = None
        for i in range(pair):
            h = p * pair + i
            w = jnp.concatenate([weights(h, at_t >= at_s), weights(heads + h, at_t <= at_s)], axis=1)
            one = dot(w, source)
            value = one if value is None else jnp.where(lane_head == i, one, value)
        inside.append(value)
    inside = jnp.concatenate(inside, axis=1)
    growth = expand(jnp.exp(l_sums))
    gate = silu(project(wz, rows))

    for copy in a_moves + t_moves:
        copy.wait()
    entering = None
    ctx_f = ctx_b = None
    for j in range(n_sp):
        mine = rcv_a[j, :, 0:inner].astype(F32)
        ctx_f = mine if ctx_f is None else ctx_f * tot[j, 0:1, 0:inner] + mine
        i = n_sp - 1 - j
        mine = rcv_a[i, :, inner:both].astype(F32)
        ctx_b = mine if ctx_b is None else ctx_b * tot[i, 0:1, inner:both] + mine
    for j in range(n_sp):
        snd_b[j, :, 0:inner] = ctx_f.astype(BF16)
        ctx_f = ctx_f * tot[j, 1:2, 0:inner] + rcv_a[j, :, both : both + inner].astype(F32)
        i = n_sp - 1 - j
        snd_b[i, :, inner:both] = ctx_b.astype(BF16)
        ctx_b = ctx_b * tot[i, 1:2, inner:both] + rcv_a[i, :, both + inner : 2 * both].astype(F32)
    b_moves = []
    for k in range(1, n_sp):
        to = lax.rem(s + k, n_sp)
        b_moves.append(remote(snd_b.at[to], rcv_b.at[s], b_send.at[k], b_recv.at[k], sp=to))
        b_moves[-1].start()
    rcv_b[s] = snd_b[s]
    for copy in b_moves:
        copy.wait()
    entering = jnp.concatenate([rcv_b[r] for r in range(n_sp)], axis=0)
    carried = dot(c_in, entering) * growth
    gated = (inside + carried[:, 0:inner] + carried[:, inner:both]) * gate
    ny = (
        gated
        * lax.rsqrt(jnp.mean(gated * gated, axis=1, keepdims=True) + EPSILON)
        * out_gain[...].astype(F32)
    ).astype(BF16)

    chunks = n_tp
    chunk = width // chunks
    o_moves = []
    for c in range(chunks):
        cut = slice(c * chunk, (c + 1) * chunk)
        result = dot(ny, wo[:, cut]).astype(BF16)
        for u in range(n_tp):
            snd_o[c, u] = result[u * own_rows : (u + 1) * own_rows]
        for k in range(1, n_tp):
            to = lax.rem(t + k, n_tp)
            at = c * n_tp + k
            o_moves.append(remote(snd_o.at[c, to], rcv_o.at[c, k], o_send.at[at], o_recv.at[at], tp=to))
            o_moves[-1].start()
    for c in range(chunks):
        mixed = snd_o[c, t].astype(F32)
        for k in range(1, n_tp):
            o_moves[c * (n_tp - 1) + k - 1].wait()
            mixed = mixed + rcv_o[c, k].astype(F32)
        out[:, c * chunk : (c + 1) * chunk] = (mods[c][4:5] * mixed).astype(BF16)


def shards(
    latent,
    condition,
    context,
    context_source,
    mod_weight,
    norm_gain,
    w_x,
    w_b,
    w_c,
    w_z,
    w_dt,
    conv_x,
    conv_b,
    conv_c,
    decay_rate,
    out_gain,
    w_out,
):
    n_sp, n_tp, n_dp = lax.axis_size("sp"), lax.axis_size("tp"), lax.axis_size("dp")
    own_rows, width = latent.shape[1:]
    ctx_rows = context.shape[1]
    depth = mod_weight.shape[1]
    cols = mod_weight.shape[2]
    inner = w_x.shape[1]
    heads = decay_rate.shape[1]
    both = 2 * inner
    rows = n_tp * own_rows
    state_rows = STATE // n_sp
    chunk = width // n_tp
    acts = jnp.stack([condition[0], context_source])
    acts = lax.dynamic_slice_in_dim(acts, lax.axis_index("sp") * depth, depth, 1)
    acts = jnp.pad(jax.nn.silu(acts.astype(F32)).astype(BF16), ((0, PAD - 2), (0, 0)))
    edges = jnp.stack([latent[0, 0], latent[0, -1], context[0, 0], context[0, -1]])
    edges = edges.astype(F32)[:, None, :]
    dt = jnp.concatenate([w_dt[0], w_dt[1]], axis=1)
    dt = jnp.pad(dt, ((0, 0), (0, LANES - 2 * heads)))
    rate = jnp.pad(decay_rate.reshape(1, 2 * heads), ((0, 0), (0, LANES - 2 * heads)))
    vmem = pl.BlockSpec(memory_space=pltpu.VMEM)
    anywhere = pl.BlockSpec(memory_space=pl.ANY)
    dma = pltpu.SemaphoreType.DMA
    scratch = [
        pltpu.VMEM((n_tp, own_rows, width), BF16),
        pltpu.VMEM((ctx_rows, width), BF16),
        pltpu.VMEM(mod_weight.shape, BF16),
        pltpu.VMEM((w_x.shape[0] * n_dp, inner), BF16),
        pltpu.VMEM((w_b.shape[0] * n_dp, w_b.shape[1]), BF16),
        pltpu.VMEM((w_c.shape[0] * n_dp, w_c.shape[1]), BF16),
        pltpu.VMEM((dt.shape[0] * n_dp, LANES), BF16),
        pltpu.VMEM((w_z.shape[0] * n_dp, inner), BF16),
        pltpu.VMEM((w_out.shape[0] * n_dp, width), BF16),
        pltpu.VMEM((8, cols), F32),
        pltpu.VMEM((n_sp, 8, cols), F32),
        pltpu.VMEM((n_tp, 8, cols), F32),
        pltpu.VMEM((4, 1, width), F32),
        pltpu.VMEM((rows + PAD + ctx_rows, width), BF16),
        pltpu.VMEM((n_sp, state_rows, 2 * both), BF16),
        pltpu.VMEM((n_sp, state_rows, 2 * both), BF16),
        pltpu.VMEM((n_sp, 8, both), F32),
        pltpu.VMEM((n_sp, state_rows, both), BF16),
        pltpu.VMEM((n_sp, state_rows, both), BF16),
        pltpu.VMEM((n_tp, n_tp, own_rows, chunk), BF16),
        pltpu.VMEM((n_tp, n_tp, own_rows, chunk), BF16),
        dma((9,)),
        dma((6 * n_dp,)),
        dma((6 * n_dp,)),
        dma((n_tp,)),
        dma((n_tp,)),
        dma((n_sp,)),
        dma((n_sp,)),
        dma((n_tp,)),
        dma((n_tp,)),
        dma((2 + 2 * n_tp,)),
        dma((4,)),
        dma((n_sp,)),
        dma((n_sp,)),
        dma((n_sp,)),
        dma((n_sp,)),
        dma((n_sp,)),
        dma((n_sp,)),
        dma((n_tp * n_tp,)),
        dma((n_tp * n_tp,)),
    ]
    result = pl.pallas_call(
        functools.partial(kernel, n_sp, n_tp, n_dp, heads),
        out_shape=jax.ShapeDtypeStruct((own_rows, width), BF16),
        in_specs=[vmem] * 8 + [anywhere] * 9,
        out_specs=vmem,
        scratch_shapes=scratch,
        compiler_params=pltpu.CompilerParams(
            has_side_effects=True, vmem_limit_bytes=62_000_000
        ),
    )(
        acts,
        edges,
        norm_gain[None],
        conv_x,
        conv_b,
        conv_c,
        rate,
        out_gain[None],
        latent[0],
        context[0],
        mod_weight,
        w_x,
        w_b,
        w_c,
        dt,
        w_z,
        w_out,
    )
    return result[None]


def solution(mesh):
    placed = (
        P("dp", ("sp", "tp"), None),
        P("dp", None),
        P("dp", "sp", None),
        P(),
        P(None, "sp", "tp"),
        P(),
        P("dp", "tp"),
        P("dp", "tp"),
        P("dp", "tp"),
        P("dp", "tp"),
        P(None, "dp", "tp"),
        P(None, "tp"),
        P(None, "tp"),
        P(None, "tp"),
        P(None, "tp"),
        P("tp"),
        P(("tp", "dp"), None),
    )
    return jax.shard_map(
        shards, mesh=mesh, in_specs=placed, out_specs=P("dp", ("sp", "tp"), None), check_vma=False
    )
```

```python
import functools

import jax
import jax.numpy as jnp
from jax import lax
from jax.experimental import pallas as pl
from jax.experimental.pallas import tpu as pltpu
from jax.sharding import PartitionSpec as P

STATE = 128
LANES = 128
PAD = 16
EPSILON = 1e-06
MESH = pl.DeviceIdType.MESH
F32 = jnp.float32
BF16 = jnp.bfloat16


def silu(v):
    return v / (1.0 + jnp.exp(-v))


def softplus(v):
    return jnp.maximum(v, 0.0) + jnp.log1p(jnp.exp(-jnp.abs(v)))


def row_of(ref):
    return ref[...].astype(F32).reshape(1, ref.shape[0])


def dot(a, b, dims=((1,), (0,)), precision=None):
    return lax.dot_general(a, b, (dims, ((), ())), precision=precision, preferred_element_type=F32)


def kernel(
    n_sp,
    n_tp,
    n_dp,
    heads,
    condition,
    source,
    gain,
    conv_x,
    conv_b,
    conv_c,
    rate,
    out_gain,
    latent,
    context,
    mod_weight,
    w_x,
    w_b,
    w_c,
    w_dt,
    w_z,
    w_out,
    out,
    lat_all,
    ctx_buf,
    mod_buf,
    wx,
    wb,
    wc,
    wd,
    wz,
    wo,
    acts,
    edges,
    part,
    part_all,
    mods,
    halo,
    hid,
    snd_a,
    rcv_a,
    tot,
    snd_b,
    rcv_b,
    snd_o,
    rcv_o,
    local_sem,
    dp_send,
    dp_recv,
    lat_send,
    lat_recv,
    mod1_send,
    mod1_recv,
    mod2_send,
    mod2_recv,
    edge_send,
    edge_recv,
    a_send,
    a_recv,
    t_send,
    t_recv,
    b_send,
    b_recv,
    o_send,
    o_recv,
):
    s = lax.axis_index("sp")
    t = lax.axis_index("tp")
    d = lax.axis_index("dp")
    own_rows, width = latent.shape
    ctx_rows = context.shape[0]
    depth = mod_weight.shape[1]
    rows = n_tp * own_rows
    inner = w_x.shape[1]
    both = 2 * inner
    head_dim = inner // heads
    nh2 = 2 * heads

    def remote(src, dst, send, recv, **to):
        return pltpu.make_async_remote_copy(
            src_ref=src, dst_ref=dst, send_sem=send, recv_sem=recv, device_id=to, device_id_type=MESH
        )

    local = []

    def fetch(src, dst):
        copy = pltpu.make_async_copy(src, dst, local_sem.at[len(local)])
        copy.start()
        local.append(copy)
        return copy

    mod_copy = fetch(mod_weight, mod_buf)
    lat_copy = fetch(latent, lat_all.at[t])
    ctx_copy = fetch(context, ctx_buf)
    lat_moves = []
    for k in range(1, n_tp):
        lat_moves.append(
            remote(latent, lat_all.at[t], lat_send.at[k], lat_recv.at[k], tp=lax.rem(t + k, n_tp))
        )
        lat_moves[-1].start()
    weight_moves = []
    pairs = ((w_x, wx), (w_b, wb), (w_dt, wd), (w_c, wc), (w_z, wz), (w_out, wo))
    for i, (src, dst) in enumerate(pairs):
        count = src.shape[0]
        place = dst.at[d] if src is w_dt else dst.at[pl.ds(d * count, count)]
        for k in range(1, n_dp):
            at = i * n_dp + k
            weight_moves.append(
                remote(src, place, dp_send.at[at], dp_recv.at[at], dp=lax.rem(d + k, n_dp))
            )
            weight_moves[-1].start()
        fetch(src, place)

    active = silu(jnp.concatenate([condition[...].astype(F32), row_of(source)], axis=0))
    for j in range(n_sp):
        acts[j, 0:2] = active[:, j * depth : (j + 1) * depth]
    own_acts = jnp.concatenate([acts[s, 0:2], jnp.zeros((PAD - 2, depth), F32)], axis=0).astype(BF16)
    mod_copy.wait()
    pieces = [dot(own_acts, mod_buf[k])[0:2] for k in range(mod_buf.shape[0])]
    cols = pieces[0].shape[1]
    part[...] = jnp.concatenate(pieces + [jnp.zeros((2, cols), F32)], axis=0)
    moves = []
    for k in range(1, n_sp):
        moves.append(
            remote(part, part_all.at[k], mod1_send.at[k], mod1_recv.at[k], sp=lax.rem(s + k, n_sp))
        )
        moves[-1].start()
    lat_copy.wait()
    edges[0] = lat_all[t, 0:1].astype(F32)
    edges[1] = lat_all[t, own_rows - 1 : own_rows].astype(F32)
    ctx_copy.wait()
    edges[2] = ctx_buf[0:1].astype(F32)
    edges[3] = ctx_buf[ctx_rows - 1 : ctx_rows].astype(F32)
    up, down = lax.rem(s + 1, n_sp), lax.rem(s + n_sp - 1, n_sp)
    ctx_up = remote(edges.at[3], halo.at[2], edge_send.at[0], edge_recv.at[2], sp=up)
    ctx_down = remote(edges.at[2], halo.at[3], edge_send.at[1], edge_recv.at[3], sp=down)
    ctx_up.start()
    ctx_down.start()
    lat_up = [
        remote(edges.at[1], halo.at[0], edge_send.at[2 + u], edge_recv.at[0], sp=up, tp=u)
        for u in range(n_tp)
    ]
    lat_down = [
        remote(edges.at[0], halo.at[1], edge_send.at[2 + n_tp + u], edge_recv.at[1], sp=down, tp=u)
        for u in range(n_tp)
    ]

    @pl.when(t == n_tp - 1)
    def _():
        for copy in lat_up:
            copy.start()

    @pl.when(t == 0)
    def _():
        for copy in lat_down:
            copy.start()

    summed = part[...]
    for k in range(1, n_sp):
        moves[k - 1].wait()
        summed = summed + part_all[k]
    mods[t] = summed
    moves = []
    for k in range(1, n_tp):
        moves.append(
            remote(mods.at[t], mods.at[t], mod2_send.at[k], mod2_recv.at[k], tp=lax.rem(t + k, n_tp))
        )
        moves[-1].start()
    for copy in moves:
        copy.wait()

    def vector(row):
        return jnp.concatenate([mods[c][row : row + 1] for c in range(n_tp)], axis=1)

    def normed(v, gains, shift):
        return v * lax.rsqrt(jnp.mean(v * v, axis=1, keepdims=True) + EPSILON) * gains + shift

    gain_row = row_of(gain)
    lat_shift, ctx_shift = vector(0), vector(1)
    lat_gain = gain_row * (1.0 + vector(2))
    ctx_gain = gain_row * (1.0 + vector(3))
    step_rows = min(32, ctx_rows)
    for r in range(0, ctx_rows, step_rows):
        block = ctx_buf[r : r + step_rows].astype(F32)
        hid[rows + PAD + r : rows + PAD + r + step_rows] = normed(block, ctx_gain, ctx_shift).astype(BF16)
    for copy in lat_moves:
        copy.wait()
    for u in range(n_tp):
        hid[u * own_rows : (u + 1) * own_rows] = normed(
            lat_all[u].astype(F32), lat_gain, lat_shift
        ).astype(BF16)
    ctx_up.wait_send()
    ctx_down.wait_send()
    ctx_up.wait_recv()
    ctx_down.wait_recv()
    lat_up[0].wait_recv()
    lat_down[0].wait_recv()

    @pl.when(t == n_tp - 1)
    def _():
        for copy in lat_up:
            copy.wait_send()

    @pl.when(t == 0)
    def _():
        for copy in lat_down:
            copy.wait_send()

    hid[rows : rows + PAD] = jnp.concatenate(
        [
            normed(halo[0], lat_gain, lat_shift),
            normed(halo[1], lat_gain, lat_shift),
            normed(halo[2], ctx_gain, ctx_shift),
            normed(halo[3], ctx_gain, ctx_shift),
            jnp.zeros((PAD - 4, width), F32),
        ],
        axis=0,
    ).astype(BF16)
    for copy in weight_moves:
        copy.wait()
    for copy in local[3:]:
        copy.wait()

    has_before = s > 0
    has_after = s < n_sp - 1

    def shaped(values, before, after, taps):
        count = values.shape[0]
        at = lax.broadcasted_iota(jnp.int32, values.shape, 0)
        before = jnp.where(has_before, before, 0.0)
        after = jnp.where(has_after, after, 0.0)
        earlier = jnp.where(at == 0, before, pltpu.roll(values, 1, 0))
        later = jnp.where(at == count - 1, after, pltpu.roll(values, count - 1, 0))
        w = taps[...].astype(F32)
        return silu(earlier * w[0:1] + values * w[1:2] + later * w[2:3]).astype(BF16)

    def project(weight, count):
        return dot(hid[0:count], weight[...]).astype(BF16).astype(F32)

    total = rows + PAD + ctx_rows
    px = project(wx, total)
    x_in = shaped(px[0:rows], px[rows : rows + 1], px[rows + 1 : rows + 2], conv_x).astype(F32)
    cx_in = shaped(
        px[rows + PAD :], px[rows + 2 : rows + 3], px[rows + 3 : rows + 4], conv_x
    ).astype(F32)
    pb = project(wb, total)
    b_in = shaped(pb[0:rows], pb[rows : rows + 1], pb[rows + 1 : rows + 2], conv_b)
    cb_in = shaped(pb[rows + PAD :], pb[rows + 2 : rows + 3], pb[rows + 3 : rows + 4], conv_b)
    features = None
    half = wd.shape[3]
    for r in range(n_dp):
        taps = jnp.concatenate(
            [wd[r, 0].astype(F32), wd[r, 1].astype(F32), jnp.zeros((LANES - nh2, half), F32)], axis=0
        ).astype(BF16)
        one = dot(hid[0:total, r * half : (r + 1) * half], taps, ((1,), (1,)))
        features = one if features is None else features + one
    step_all = softplus(features.astype(BF16).astype(F32))
    rates = jnp.concatenate([rate[0:1], rate[1:2], jnp.zeros((1, LANES - nh2), F32)], axis=1)

    spread_at = lax.broadcasted_iota(jnp.int32, (LANES, both), 0)
    spread_to = lax.broadcasted_iota(jnp.int32, (LANES, both), 1) // head_dim
    spreader = jnp.where((spread_to == spread_at) | (spread_to + nh2 == spread_at), 1.0, 0.0).astype(BF16)

    def expand(v):
        lane = lax.broadcasted_iota(jnp.int32, v.shape, 1)
        high = v.astype(BF16).astype(F32)
        low = pltpu.roll(v - high, nh2, 1)
        packed = jnp.where(lane < nh2, high, jnp.where(lane < 2 * nh2, low, 0.0))
        return dot(packed.astype(BF16), spreader)

    def running(steps):
        count = steps.shape[0]
        logs = -rates * steps
        a = lax.broadcasted_iota(jnp.int32, (count, count), 0)
        b = lax.broadcasted_iota(jnp.int32, (count, count), 1)
        lower = jnp.where(a >= b, 1.0, 0.0)
        upper = jnp.where(a <= b, 1.0, 0.0)
        lane = lax.broadcasted_iota(jnp.int32, logs.shape, 1)
        sums = jnp.where(
            lane < heads,
            dot(lower, logs, precision=lax.Precision.HIGHEST),
            dot(upper, logs, precision=lax.Precision.HIGHEST),
        )
        row_lane = lax.broadcasted_iota(jnp.int32, (1, LANES), 1)
        ends = jnp.where(row_lane < heads, sums[count - 1 : count], sums[0:1])
        return sums, ends

    def moved(values, steps):
        wide = jnp.concatenate([values, values], axis=1)
        return (wide * expand(steps)).astype(BF16)

    c_steps = step_all[rows + PAD :]
    c_sums, c_ends = running(c_steps)
    c_moved = moved(cx_in, c_steps)
    c_scaled = (c_moved.astype(F32) * expand(jnp.exp(c_ends - c_sums))).astype(BF16)
    c_state = dot(cb_in, c_scaled, ((0,), (0,)))
    l_steps = step_all[0:rows]
    l_sums, l_ends = running(l_steps)
    l_moved = moved(x_in, l_steps)
    l_scaled = (l_moved.astype(F32) * expand(jnp.exp(l_ends - l_sums))).astype(BF16)
    l_state = dot(b_in, l_scaled, ((0,), (0,)))
    state_rows = STATE // n_sp
    for r in range(n_sp):
        cut = slice(r * state_rows, (r + 1) * state_rows)
        snd_a[r, :, 0:both] = c_state[cut].astype(BF16)
        snd_a[r, :, both : 2 * both] = l_state[cut].astype(BF16)
    ends = jnp.exp(jnp.concatenate([c_ends, l_ends, jnp.zeros((6, LANES), F32)], axis=0))
    tot[s] = expand(ends)
    a_moves, t_moves = [], []
    for k in range(1, n_sp):
        to = lax.rem(s + k, n_sp)
        a_moves.append(remote(snd_a.at[to], rcv_a.at[s], a_send.at[k], a_recv.at[k], sp=to))
        a_moves[-1].start()
        t_moves.append(remote(tot.at[s], tot.at[s], t_send.at[k], t_recv.at[k], sp=to))
        t_moves[-1].start()
    rcv_a[s] = snd_a[s]

    pc = project(wc, rows + PAD)
    c_in = shaped(pc[0:rows], pc[rows : rows + 1], pc[rows + 1 : rows + 2], conv_c)
    scores = dot(c_in, b_in, ((1,), (1,)))
    at_t = lax.broadcasted_iota(jnp.int32, (rows, rows), 0)
    at_s = lax.broadcasted_iota(jnp.int32, (rows, rows), 1)
    sums_t = jnp.transpose(l_sums)

    def weights(lane, keep):
        gap = l_sums[:, lane : lane + 1] - sums_t[lane : lane + 1]
        return jnp.where(keep, scores * jnp.exp(jnp.minimum(gap, 0.0)), 0.0).astype(BF16)

    pair = LANES // head_dim
    inside = []
    lane_head = lax.broadcasted_iota(jnp.int32, (rows, LANES), 1) // head_dim
    for p in range(heads // pair):
        cut = slice(p * LANES, (p + 1) * LANES)
        cut_b = slice(inner + p * LANES, inner + (p + 1) * LANES)
        source = jnp.concatenate([l_moved[:, cut], l_moved[:, cut_b]], axis=0)
        value = None
        for i in range(pair):
            h = p * pair + i
            w = jnp.concatenate([weights(h, at_t >= at_s), weights(heads + h, at_t <= at_s)], axis=1)
            one = dot(w, source)
            value = one if value is None else jnp.where(lane_head == i, one, value)
        inside.append(value)
    inside = jnp.concatenate(inside, axis=1)
    growth = expand(jnp.exp(l_sums))
    gate = silu(project(wz, rows))

    for copy in a_moves + t_moves:
        copy.wait()
    entering = None
    ctx_f = ctx_b = None
    for j in range(n_sp):
        mine = rcv_a[j, :, 0:inner].astype(F32)
        ctx_f = mine if ctx_f is None else ctx_f * tot[j, 0:1, 0:inner] + mine
        i = n_sp - 1 - j
        mine = rcv_a[i, :, inner:both].astype(F32)
        ctx_b = mine if ctx_b is None else ctx_b * tot[i, 0:1, inner:both] + mine
    for j in range(n_sp):
        snd_b[j, :, 0:inner] = ctx_f.astype(BF16)
        ctx_f = ctx_f * tot[j, 1:2, 0:inner] + rcv_a[j, :, both : both + inner].astype(F32)
        i = n_sp - 1 - j
        snd_b[i, :, inner:both] = ctx_b.astype(BF16)
        ctx_b = ctx_b * tot[i, 1:2, inner:both] + rcv_a[i, :, both + inner : 2 * both].astype(F32)
    b_moves = []
    for k in range(1, n_sp):
        to = lax.rem(s + k, n_sp)
        b_moves.append(remote(snd_b.at[to], rcv_b.at[s], b_send.at[k], b_recv.at[k], sp=to))
        b_moves[-1].start()
    rcv_b[s] = snd_b[s]
    for copy in b_moves:
        copy.wait()
    entering = jnp.concatenate([rcv_b[r] for r in range(n_sp)], axis=0)
    carried = dot(c_in, entering) * growth
    gated = (inside + carried[:, 0:inner] + carried[:, inner:both]) * gate
    ny = (
        gated
        * lax.rsqrt(jnp.mean(gated * gated, axis=1, keepdims=True) + EPSILON)
        * row_of(out_gain)
    ).astype(BF16)

    chunks = n_tp
    chunk = width // chunks
    o_moves = []
    for c in range(chunks):
        cut = slice(c * chunk, (c + 1) * chunk)
        result = dot(ny, wo[:, cut]).astype(BF16)
        for u in range(n_tp):
            snd_o[c, u] = result[u * own_rows : (u + 1) * own_rows]
        for k in range(1, n_tp):
            to = lax.rem(t + k, n_tp)
            at = c * n_tp + k
            o_moves.append(remote(snd_o.at[c, to], rcv_o.at[c, k], o_send.at[at], o_recv.at[at], tp=to))
            o_moves[-1].start()
    for c in range(chunks):
        mixed = snd_o[c, t].astype(F32)
        for k in range(1, n_tp):
            o_moves[c * (n_tp - 1) + k - 1].wait()
            mixed = mixed + rcv_o[c, k].astype(F32)
        out[:, c * chunk : (c + 1) * chunk] = (mods[c][4:5] * mixed).astype(BF16)


def shards(
    latent,
    condition,
    context,
    context_source,
    mod_weight,
    norm_gain,
    w_x,
    w_b,
    w_c,
    w_z,
    w_dt,
    conv_x,
    conv_b,
    conv_c,
    decay_rate,
    out_gain,
    w_out,
):
    n_sp, n_tp, n_dp = lax.axis_size("sp"), lax.axis_size("tp"), lax.axis_size("dp")
    own_rows, width = latent.shape[1:]
    ctx_rows = context.shape[1]
    depth = mod_weight.shape[1]
    cols = mod_weight.shape[2]
    inner = w_x.shape[1]
    heads = decay_rate.shape[1]
    both = 2 * inner
    rows = n_tp * own_rows
    state_rows = STATE // n_sp
    chunk = width // n_tp
    vmem = pl.BlockSpec(memory_space=pltpu.VMEM)
    anywhere = pl.BlockSpec(memory_space=pl.ANY)
    dma = pltpu.SemaphoreType.DMA
    scratch = [
        pltpu.VMEM((n_tp, own_rows, width), BF16),
        pltpu.VMEM((ctx_rows, width), BF16),
        pltpu.VMEM(mod_weight.shape, BF16),
        pltpu.VMEM((w_x.shape[0] * n_dp, inner), BF16),
        pltpu.VMEM((w_b.shape[0] * n_dp, w_b.shape[1]), BF16),
        pltpu.VMEM((w_c.shape[0] * n_dp, w_c.shape[1]), BF16),
        pltpu.VMEM((n_dp, 2, heads, w_dt.shape[1]), BF16),
        pltpu.VMEM((w_z.shape[0] * n_dp, inner), BF16),
        pltpu.VMEM((w_out.shape[0] * n_dp, width), BF16),
        pltpu.VMEM((n_sp, 8, depth), F32),
        pltpu.VMEM((4, 1, width), F32),
        pltpu.VMEM((8, cols), F32),
        pltpu.VMEM((n_sp, 8, cols), F32),
        pltpu.VMEM((n_tp, 8, cols), F32),
        pltpu.VMEM((4, 1, width), F32),
        pltpu.VMEM((rows + PAD + ctx_rows, width), BF16),
        pltpu.VMEM((n_sp, state_rows, 2 * both), BF16),
        pltpu.VMEM((n_sp, state_rows, 2 * both), BF16),
        pltpu.VMEM((n_sp, 8, both), F32),
        pltpu.VMEM((n_sp, state_rows, both), BF16),
        pltpu.VMEM((n_sp, state_rows, both), BF16),
        pltpu.VMEM((n_tp, n_tp, own_rows, chunk), BF16),
        pltpu.VMEM((n_tp, n_tp, own_rows, chunk), BF16),
        dma((9,)),
        dma((6 * n_dp,)),
        dma((6 * n_dp,)),
        dma((n_tp,)),
        dma((n_tp,)),
        dma((n_sp,)),
        dma((n_sp,)),
        dma((n_tp,)),
        dma((n_tp,)),
        dma((2 + 2 * n_tp,)),
        dma((4,)),
        dma((n_sp,)),
        dma((n_sp,)),
        dma((n_sp,)),
        dma((n_sp,)),
        dma((n_sp,)),
        dma((n_sp,)),
        dma((n_tp * n_tp,)),
        dma((n_tp * n_tp,)),
    ]
    result = pl.pallas_call(
        functools.partial(kernel, n_sp, n_tp, n_dp, heads),
        out_shape=jax.ShapeDtypeStruct((own_rows, width), BF16),
        in_specs=[vmem] * 8 + [anywhere] * 9,
        out_specs=vmem,
        scratch_shapes=scratch,
        compiler_params=pltpu.CompilerParams(
            has_side_effects=True, vmem_limit_bytes=62_000_000
        ),
    )(
        condition,
        context_source,
        norm_gain,
        conv_x,
        conv_b,
        conv_c,
        decay_rate,
        out_gain,
        latent[0],
        context[0],
        mod_weight,
        w_x,
        w_b,
        w_c,
        jnp.swapaxes(w_dt, 1, 2),
        w_z,
        w_out,
    )
    return result[None]


def solution(mesh):
    placed = (
        P("dp", ("sp", "tp"), None),
        P("dp", None),
        P("dp", "sp", None),
        P(),
        P(None, "sp", "tp"),
        P(),
        P("dp", "tp"),
        P("dp", "tp"),
        P("dp", "tp"),
        P("dp", "tp"),
        P(None, "dp", "tp"),
        P(None, "tp"),
        P(None, "tp"),
        P(None, "tp"),
        P(None, "tp"),
        P("tp"),
        P(("tp", "dp"), None),
    )
    return jax.shard_map(
        shards, mesh=mesh, in_specs=placed, out_specs=P("dp", ("sp", "tp"), None), check_vma=False
    )
```

```python
import functools

import jax
import jax.numpy as jnp
from jax import lax
from jax.experimental import pallas as pl
from jax.experimental.pallas import tpu as pltpu
from jax.sharding import PartitionSpec as P

STATE = 128
LANES = 128
PAD = 16
EPSILON = 1e-06
MESH = pl.DeviceIdType.MESH
F32 = jnp.float32
BF16 = jnp.bfloat16


def silu(v):
    return v / (1.0 + jnp.exp(-v))


def softplus(v):
    return jnp.maximum(v, 0.0) + jnp.log1p(jnp.exp(-jnp.abs(v)))


def row_of(ref):
    return ref[...].astype(F32).reshape(1, ref.shape[0])


def dot(a, b, dims=((1,), (0,)), precision=None):
    return lax.dot_general(a, b, (dims, ((), ())), precision=precision, preferred_element_type=F32)


def kernel(
    n_sp,
    n_tp,
    n_dp,
    heads,
    condition,
    source,
    gain,
    conv_x,
    conv_b,
    conv_c,
    rate,
    out_gain,
    latent,
    context,
    mod_weight,
    w_x,
    w_b,
    w_c,
    w_dt,
    w_z,
    w_out,
    out,
    lat_all,
    ctx_buf,
    mod_buf,
    wx,
    wb,
    wc,
    wd,
    wz,
    wo,
    acts,
    edges,
    part,
    part_all,
    mods,
    halo,
    hid,
    own,
    fade,
    snd,
    rcv,
    tot,
    snd_o,
    rcv_o,
    local_sem,
    dp_send,
    dp_recv,
    lat_send,
    lat_recv,
    mod1_send,
    mod1_recv,
    mod2_send,
    mod2_recv,
    edge_send,
    edge_recv,
    chain_send,
    chain_recv,
    t_send,
    t_recv,
    o_send,
    o_recv,
):
    s = lax.axis_index("sp")
    t = lax.axis_index("tp")
    d = lax.axis_index("dp")
    own_rows, width = latent.shape
    ctx_rows = context.shape[0]
    depth = mod_weight.shape[1]
    rows = n_tp * own_rows
    inner = w_x.shape[1]
    both = 2 * inner
    head_dim = inner // heads
    nh2 = 2 * heads

    def remote(src, dst, send, recv, **to):
        return pltpu.make_async_remote_copy(
            src_ref=src, dst_ref=dst, send_sem=send, recv_sem=recv, device_id=to, device_id_type=MESH
        )

    up, down = lax.rem(s + 1, n_sp), lax.rem(s + n_sp - 1, n_sp)
    barrier = pltpu.get_barrier_semaphore()

    def greet(**to):
        pl.semaphore_signal(barrier, inc=1, device_id=to, device_id_type=MESH)

    for k in range(1, n_sp):
        greet(sp=lax.rem(s + k, n_sp))
    for k in range(1, n_tp):
        beside = lax.rem(t + k, n_tp)
        greet(tp=beside)
        greet(sp=up, tp=beside)
        greet(sp=down, tp=beside)
    for k in range(1, n_dp):
        greet(dp=lax.rem(d + k, n_dp))

    local = []

    def fetch(src, dst):
        copy = pltpu.make_async_copy(src, dst, local_sem.at[len(local)])
        copy.start()
        local.append(copy)
        return copy

    mod_copy = fetch(mod_weight, mod_buf)
    lat_copy = fetch(latent, lat_all.at[t])
    ctx_copy = fetch(context, ctx_buf)
    lat_moves = []
    for k in range(1, n_tp):
        lat_moves.append(
            remote(latent, lat_all.at[t], lat_send.at[k], lat_recv.at[k], tp=lax.rem(t + k, n_tp))
        )
    weight_moves = []
    pairs = ((w_x, wx), (w_b, wb), (w_dt, wd), (w_c, wc), (w_z, wz), (w_out, wo))
    for i, (src, dst) in enumerate(pairs):
        count = src.shape[0]
        place = dst.at[d] if src is w_dt else dst.at[pl.ds(d * count, count)]
        for k in range(1, n_dp):
            at = i * n_dp + k
            weight_moves.append(
                remote(src, place, dp_send.at[at], dp_recv.at[at], dp=lax.rem(d + k, n_dp))
            )
        fetch(src, place)

    active = silu(jnp.concatenate([condition[...].astype(F32), row_of(source)], axis=0))
    for j in range(n_sp):
        acts[j, 0:2] = active[:, j * depth : (j + 1) * depth]
    own_acts = jnp.concatenate([acts[s, 0:2], jnp.zeros((PAD - 2, depth), F32)], axis=0).astype(BF16)
    mod_copy.wait()
    pieces = [dot(own_acts, mod_buf[k])[0:2] for k in range(mod_buf.shape[0])]
    cols = pieces[0].shape[1]
    part[...] = jnp.concatenate(pieces + [jnp.zeros((2, cols), F32)], axis=0)
    pl.semaphore_wait(barrier, n_sp + 3 * n_tp + n_dp - 5)
    moves = []
    for k in range(1, n_sp):
        moves.append(
            remote(part, part_all.at[k], mod1_send.at[k], mod1_recv.at[k], sp=lax.rem(s + k, n_sp))
        )
        moves[-1].start()
    for copy in lat_moves + weight_moves:
        copy.start()
    lat_copy.wait()
    edges[0] = lat_all[t, 0:1].astype(F32)
    edges[1] = lat_all[t, own_rows - 1 : own_rows].astype(F32)
    ctx_copy.wait()
    edges[2] = ctx_buf[0:1].astype(F32)
    edges[3] = ctx_buf[ctx_rows - 1 : ctx_rows].astype(F32)
    ctx_up = remote(edges.at[3], halo.at[2], edge_send.at[0], edge_recv.at[2], sp=up)
    ctx_down = remote(edges.at[2], halo.at[3], edge_send.at[1], edge_recv.at[3], sp=down)
    ctx_up.start()
    ctx_down.start()
    lat_up = [
        remote(edges.at[1], halo.at[0], edge_send.at[2 + u], edge_recv.at[0], sp=up, tp=u)
        for u in range(n_tp)
    ]
    lat_down = [
        remote(edges.at[0], halo.at[1], edge_send.at[2 + n_tp + u], edge_recv.at[1], sp=down, tp=u)
        for u in range(n_tp)
    ]

    @pl.when(t == n_tp - 1)
    def _():
        for copy in lat_up:
            copy.start()

    @pl.when(t == 0)
    def _():
        for copy in lat_down:
            copy.start()

    summed = part[...]
    for k in range(1, n_sp):
        moves[k - 1].wait()
        summed = summed + part_all[k]
    mods[t] = summed
    moves = []
    for k in range(1, n_tp):
        moves.append(
            remote(mods.at[t], mods.at[t], mod2_send.at[k], mod2_recv.at[k], tp=lax.rem(t + k, n_tp))
        )
        moves[-1].start()
    for copy in moves:
        copy.wait()

    def vector(row):
        return jnp.concatenate([mods[c][row : row + 1] for c in range(n_tp)], axis=1)

    def normed(v, gains, shift):
        return v * lax.rsqrt(jnp.mean(v * v, axis=1, keepdims=True) + EPSILON) * gains + shift

    gain_row = row_of(gain)
    lat_shift, ctx_shift = vector(0), vector(1)
    lat_gain = gain_row * (1.0 + vector(2))
    ctx_gain = gain_row * (1.0 + vector(3))
    step_rows = min(32, ctx_rows)
    for r in range(0, ctx_rows, step_rows):
        block = ctx_buf[r : r + step_rows].astype(F32)
        hid[rows + PAD + r : rows + PAD + r + step_rows] = normed(block, ctx_gain, ctx_shift).astype(BF16)
    for copy in lat_moves:
        copy.wait()
    for u in range(n_tp):
        hid[u * own_rows : (u + 1) * own_rows] = normed(
            lat_all[u].astype(F32), lat_gain, lat_shift
        ).astype(BF16)
    ctx_up.wait_send()
    ctx_down.wait_send()
    ctx_up.wait_recv()
    ctx_down.wait_recv()
    lat_up[0].wait_recv()
    lat_down[0].wait_recv()

    @pl.when(t == n_tp - 1)
    def _():
        for copy in lat_up:
            copy.wait_send()

    @pl.when(t == 0)
    def _():
        for copy in lat_down:
            copy.wait_send()

    hid[rows : rows + PAD] = jnp.concatenate(
        [
            normed(halo[0], lat_gain, lat_shift),
            normed(halo[1], lat_gain, lat_shift),
            normed(halo[2], ctx_gain, ctx_shift),
            normed(halo[3], ctx_gain, ctx_shift),
            jnp.zeros((PAD - 4, width), F32),
        ],
        axis=0,
    ).astype(BF16)
    for copy in weight_moves:
        copy.wait()
    for copy in local[3:]:
        copy.wait()

    has_before = s > 0
    has_after = s < n_sp - 1

    def shaped(values, before, after, taps):
        count = values.shape[0]
        at = lax.broadcasted_iota(jnp.int32, values.shape, 0)
        before = jnp.where(has_before, before, 0.0)
        after = jnp.where(has_after, after, 0.0)
        earlier = jnp.where(at == 0, before, pltpu.roll(values, 1, 0))
        later = jnp.where(at == count - 1, after, pltpu.roll(values, count - 1, 0))
        w = taps[...].astype(F32)
        return silu(earlier * w[0:1] + values * w[1:2] + later * w[2:3]).astype(BF16)

    def project(weight, count):
        return dot(hid[0:count], weight[...]).astype(BF16).astype(F32)

    total = rows + PAD + ctx_rows
    features = None
    half = wd.shape[3]
    for r in range(n_dp):
        taps = jnp.concatenate(
            [wd[r, 0].astype(F32), wd[r, 1].astype(F32), jnp.zeros((LANES - nh2, half), F32)], axis=0
        ).astype(BF16)
        one = dot(hid[0:total, r * half : (r + 1) * half], taps, ((1,), (1,)))
        features = one if features is None else features + one
    step_all = softplus(features.astype(BF16).astype(F32))
    rates = jnp.concatenate([rate[0:1], rate[1:2], jnp.zeros((1, LANES - nh2), F32)], axis=1)


    def running(steps):
        count = steps.shape[0]
        logs = -rates * steps
        a = lax.broadcasted_iota(jnp.int32, (count, count), 0)
        b = lax.broadcasted_iota(jnp.int32, (count, count), 1)
        lower = jnp.where(a >= b, 1.0, 0.0)
        upper = jnp.where(a <= b, 1.0, 0.0)
        lane = lax.broadcasted_iota(jnp.int32, logs.shape, 1)
        sums = jnp.where(
            lane < heads,
            dot(lower, logs, precision=lax.Precision.HIGHEST),
            dot(upper, logs, precision=lax.Precision.HIGHEST),
        )
        row_lane = lax.broadcasted_iota(jnp.int32, (1, LANES), 1)
        ends = jnp.where(row_lane < heads, sums[count - 1 : count], sums[0:1])
        return sums, ends

    c_steps = step_all[rows + PAD :]
    c_sums, c_ends = running(c_steps)
    l_steps = step_all[0:rows]
    l_sums, l_ends = running(l_steps)
    tot[s] = jnp.concatenate([c_ends, l_ends, jnp.zeros((6, LANES), F32)], axis=0)
    t_moves = []
    for k in range(1, n_sp):
        to = lax.rem(s + k, n_sp)
        t_moves.append(remote(tot.at[s], tot.at[s], t_send.at[k], t_recv.at[k], sp=to))
        t_moves[-1].start()

    px = project(wx, total)
    x_in = shaped(px[0:rows], px[rows : rows + 1], px[rows + 1 : rows + 2], conv_x).astype(F32)
    cx_in = shaped(
        px[rows + PAD :], px[rows + 2 : rows + 3], px[rows + 3 : rows + 4], conv_x
    ).astype(F32)
    pb = project(wb, total)
    b_in = shaped(pb[0:rows], pb[rows : rows + 1], pb[rows + 1 : rows + 2], conv_b)
    cb_in = shaped(pb[rows + PAD :], pb[rows + 2 : rows + 3], pb[rows + 3 : rows + 4], conv_b)
    spread_at = lax.broadcasted_iota(jnp.int32, (LANES, both), 0)
    spread_to = lax.broadcasted_iota(jnp.int32, (LANES, both), 1) // head_dim
    spreader = jnp.where((spread_to == spread_at) | (spread_to + nh2 == spread_at), 1.0, 0.0).astype(BF16)

    def expand(v):
        lane = lax.broadcasted_iota(jnp.int32, v.shape, 1)
        high = v.astype(BF16).astype(F32)
        low = pltpu.roll(v - high, nh2, 1)
        packed = jnp.where(lane < nh2, high, jnp.where(lane < 2 * nh2, low, 0.0))
        return dot(packed.astype(BF16), spreader)

    def moved(values, steps):
        wide = jnp.concatenate([values, values], axis=1)
        return (wide * expand(steps)).astype(BF16)

    c_moved = moved(cx_in, c_steps)
    c_scaled = (c_moved.astype(F32) * expand(jnp.exp(c_ends - c_sums))).astype(BF16)
    c_state = dot(cb_in, c_scaled, ((0,), (0,)))
    l_moved = moved(x_in, l_steps)
    l_scaled = (l_moved.astype(F32) * expand(jnp.exp(l_ends - l_sums))).astype(BF16)
    l_state = dot(b_in, l_scaled, ((0,), (0,)))
    for copy in t_moves:
        copy.wait()
    row_lane = lax.broadcasted_iota(jnp.int32, (1, LANES), 1)
    c_later = jnp.zeros((1, LANES), F32)
    l_earlier = jnp.zeros((1, LANES), F32)
    for j in range(n_sp):
        left = jnp.where(row_lane < heads, 1, 0) * (s > j).astype(jnp.int32)
        left = left + jnp.where(row_lane < heads, 0, 1) * (s < j).astype(jnp.int32)
        right = jnp.where(row_lane < heads, 1, 0) * (s < j).astype(jnp.int32)
        right = right + jnp.where(row_lane < heads, 0, 1) * (s > j).astype(jnp.int32)
        c_later = c_later + jnp.where(right > 0, tot[j, 0:1], 0.0)
        l_earlier = l_earlier + jnp.where(left > 0, tot[j, 1:2], 0.0)
    fades = expand(
        jnp.exp(
            jnp.concatenate(
                [c_later, l_earlier, l_ends, l_earlier + l_ends, jnp.zeros((4, LANES), F32)], axis=0
            )
        )
    )
    c_state = c_state * fades[0:1]
    l_state = l_state + c_state * fades[3:4]
    cuts = inner // LANES
    for q in range(2):
        for c in range(cuts):
            at = q * inner + c * LANES
            apart = (1 - q) * inner + c * LANES
            own[q, 2 * c] = l_state[:, at : at + LANES]
            own[q, 2 * c + 1] = c_state[:, apart : apart + LANES]
            fade[q, 2 * c, 0:1] = fades[2:3, at : at + LANES]
            fade[q, 2 * c + 1, 0:1] = jnp.ones((1, LANES), F32)

    ends_chain = (s == 0) | (s == n_sp - 1)
    near = jnp.where(2 * s < n_sp, 0, 1)
    far = 1 - near
    messages = 2 * cuts

    def comes(q):
        return jnp.where(q == 0, s, n_sp - 1 - s) > 0

    def goes(q):
        return jnp.where(q == 0, n_sp - 1 - s, s) > 0

    def message(q, m):
        to = jnp.where(q == 0, up, down)
        return remote(snd.at[q, m], rcv.at[q, m], chain_send.at[q, m], chain_recv.at[q, m], sp=to)

    def hop(q, m):
        @pl.when(comes(q))
        def _():
            message(q, m).wait_recv()

        @pl.when(goes(q))
        def _():
            snd[q, m] = (own[q, m] + rcv[q, m].astype(F32) * fade[q, m, 0:1]).astype(BF16)
            message(q, m).start()

    for q in range(2):

        @pl.when(jnp.logical_not(comes(q)))
        def _():
            rcv[q] = jnp.zeros(rcv.shape[1:], BF16)

    @pl.when(ends_chain)
    def _():
        for m in range(messages):
            hop(near, m)

    pc = project(wc, rows + PAD)
    c_in = shaped(pc[0:rows], pc[rows : rows + 1], pc[rows + 1 : rows + 2], conv_c)
    scores = dot(c_in, b_in, ((1,), (1,)))
    at_t = lax.broadcasted_iota(jnp.int32, (rows, rows), 0)
    at_s = lax.broadcasted_iota(jnp.int32, (rows, rows), 1)
    sums_t = jnp.transpose(l_sums)

    def weights(lane, keep):
        gap = l_sums[:, lane : lane + 1] - sums_t[lane : lane + 1]
        return jnp.where(keep, scores * jnp.exp(jnp.minimum(gap, 0.0)), 0.0).astype(BF16)

    pair = LANES // head_dim
    inside = []
    lane_head = lax.broadcasted_iota(jnp.int32, (rows, LANES), 1) // head_dim
    for p in range(heads // pair):
        cut = slice(p * LANES, (p + 1) * LANES)
        cut_b = slice(inner + p * LANES, inner + (p + 1) * LANES)
        source = jnp.concatenate([l_moved[:, cut], l_moved[:, cut_b]], axis=0)
        value = None
        for i in range(pair):
            h = p * pair + i
            w = jnp.concatenate([weights(h, at_t >= at_s), weights(heads + h, at_t <= at_s)], axis=1)
            one = dot(w, source)
            value = one if value is None else jnp.where(lane_head == i, one, value)
        inside.append(value)
    inside = jnp.concatenate(inside, axis=1)
    growth = expand(jnp.exp(l_sums))
    gate = silu(project(wz, rows))

    lag = messages // 2

    @pl.when(jnp.logical_not(ends_chain))
    def _():
        for m in range(messages + lag):
            if m < messages:
                hop(near, m)
            if m >= lag:
                hop(far, m - lag)

    @pl.when(ends_chain)
    def _():
        for m in range(messages):
            hop(far, m)

    entering = []
    for q in range(2):
        for c in range(cuts):
            at = q * inner + c * LANES
            context_sum = own[1 - q, 2 * c + 1] + rcv[1 - q, 2 * c + 1].astype(F32)
            entering.append(
                (rcv[q, 2 * c].astype(F32) + context_sum * fades[1:2, at : at + LANES]).astype(BF16)
            )
    entering = jnp.concatenate(entering, axis=1)
    carried = dot(c_in, entering) * growth
    gated = (inside + carried[:, 0:inner] + carried[:, inner:both]) * gate
    ny = (
        gated
        * lax.rsqrt(jnp.mean(gated * gated, axis=1, keepdims=True) + EPSILON)
        * row_of(out_gain)
    ).astype(BF16)

    chunks = n_tp
    chunk = width // chunks
    o_moves = []
    for c in range(chunks):
        cut = slice(c * chunk, (c + 1) * chunk)
        result = dot(ny, wo[:, cut]).astype(BF16)
        for u in range(n_tp):
            snd_o[c, u] = result[u * own_rows : (u + 1) * own_rows]
        for k in range(1, n_tp):
            to = lax.rem(t + k, n_tp)
            at = c * n_tp + k
            o_moves.append(remote(snd_o.at[c, to], rcv_o.at[c, k], o_send.at[at], o_recv.at[at], tp=to))
            o_moves[-1].start()
    for q in range(2):

        @pl.when(goes(q))
        def _():
            for m in range(messages):
                message(q, m).wait_send()

    for c in range(chunks):
        mixed = snd_o[c, t].astype(F32)
        for k in range(1, n_tp):
            o_moves[c * (n_tp - 1) + k - 1].wait()
            mixed = mixed + rcv_o[c, k].astype(F32)
        out[:, c * chunk : (c + 1) * chunk] = (mods[c][4:5] * mixed).astype(BF16)


def shards(
    latent,
    condition,
    context,
    context_source,
    mod_weight,
    norm_gain,
    w_x,
    w_b,
    w_c,
    w_z,
    w_dt,
    conv_x,
    conv_b,
    conv_c,
    decay_rate,
    out_gain,
    w_out,
):
    n_sp, n_tp, n_dp = lax.axis_size("sp"), lax.axis_size("tp"), lax.axis_size("dp")
    own_rows, width = latent.shape[1:]
    ctx_rows = context.shape[1]
    depth = mod_weight.shape[1]
    cols = mod_weight.shape[2]
    inner = w_x.shape[1]
    heads = decay_rate.shape[1]
    both = 2 * inner
    rows = n_tp * own_rows
    messages = 2 * (inner // LANES)
    chunk = width // n_tp
    vmem = pl.BlockSpec(memory_space=pltpu.VMEM)
    anywhere = pl.BlockSpec(memory_space=pl.ANY)
    dma = pltpu.SemaphoreType.DMA
    scratch = [
        pltpu.VMEM((n_tp, own_rows, width), BF16),
        pltpu.VMEM((ctx_rows, width), BF16),
        pltpu.VMEM(mod_weight.shape, BF16),
        pltpu.VMEM((w_x.shape[0] * n_dp, inner), BF16),
        pltpu.VMEM((w_b.shape[0] * n_dp, w_b.shape[1]), BF16),
        pltpu.VMEM((w_c.shape[0] * n_dp, w_c.shape[1]), BF16),
        pltpu.VMEM((n_dp, 2, heads, w_dt.shape[1]), BF16),
        pltpu.VMEM((w_z.shape[0] * n_dp, inner), BF16),
        pltpu.VMEM((w_out.shape[0] * n_dp, width), BF16),
        pltpu.VMEM((n_sp, 8, depth), F32),
        pltpu.VMEM((4, 1, width), F32),
        pltpu.VMEM((8, cols), F32),
        pltpu.VMEM((n_sp, 8, cols), F32),
        pltpu.VMEM((n_tp, 8, cols), F32),
        pltpu.VMEM((4, 1, width), F32),
        pltpu.VMEM((rows + PAD + ctx_rows, width), BF16),
        pltpu.VMEM((2, messages, STATE, LANES), F32),
        pltpu.VMEM((2, messages, 8, LANES), F32),
        pltpu.VMEM((2, messages, STATE, LANES), BF16),
        pltpu.VMEM((2, messages, STATE, LANES), BF16),
        pltpu.VMEM((n_sp, 8, LANES), F32),
        pltpu.VMEM((n_tp, n_tp, own_rows, chunk), BF16),
        pltpu.VMEM((n_tp, n_tp, own_rows, chunk), BF16),
        dma((9,)),
        dma((6 * n_dp,)),
        dma((6 * n_dp,)),
        dma((n_tp,)),
        dma((n_tp,)),
        dma((n_sp,)),
        dma((n_sp,)),
        dma((n_tp,)),
        dma((n_tp,)),
        dma((2 + 2 * n_tp,)),
        dma((4,)),
        dma((2, messages)),
        dma((2, messages)),
        dma((n_sp,)),
        dma((n_sp,)),
        dma((n_tp * n_tp,)),
        dma((n_tp * n_tp,)),
    ]
    result = pl.pallas_call(
        functools.partial(kernel, n_sp, n_tp, n_dp, heads),
        out_shape=jax.ShapeDtypeStruct((own_rows, width), BF16),
        in_specs=[vmem] * 8 + [anywhere] * 9,
        out_specs=vmem,
        scratch_shapes=scratch,
        compiler_params=pltpu.CompilerParams(
            has_side_effects=True, collective_id=0, vmem_limit_bytes=62_000_000
        ),
    )(
        condition,
        context_source,
        norm_gain,
        conv_x,
        conv_b,
        conv_c,
        decay_rate,
        out_gain,
        latent[0],
        context[0],
        mod_weight,
        w_x,
        w_b,
        w_c,
        jnp.swapaxes(w_dt, 1, 2),
        w_z,
        w_out,
    )
    return result[None]


def solution(mesh):
    placed = (
        P("dp", ("sp", "tp"), None),
        P("dp", None),
        P("dp", "sp", None),
        P(),
        P(None, "sp", "tp"),
        P(),
        P("dp", "tp"),
        P("dp", "tp"),
        P("dp", "tp"),
        P("dp", "tp"),
        P(None, "dp", "tp"),
        P(None, "tp"),
        P(None, "tp"),
        P(None, "tp"),
        P(None, "tp"),
        P("tp"),
        P(("tp", "dp"), None),
    )
    return jax.shard_map(
        shards, mesh=mesh, in_specs=placed, out_specs=P("dp", ("sp", "tp"), None), check_vma=False
    )
```

```python
import functools

import jax
import jax.numpy as jnp
from jax import lax
from jax.experimental import pallas as pl
from jax.experimental.pallas import tpu as pltpu
from jax.sharding import PartitionSpec as P

STATE = 128
LANES = 128
PAD = 16
EPSILON = 1e-06
MESH = pl.DeviceIdType.MESH
F32 = jnp.float32
BF16 = jnp.bfloat16


def silu(v):
    return v / (1.0 + jnp.exp(-v))


def softplus(v):
    return jnp.maximum(v, 0.0) + jnp.log1p(jnp.exp(-jnp.abs(v)))


def row_of(ref):
    return ref[...].astype(F32).reshape(1, ref.shape[0])


def dot(a, b, dims=((1,), (0,)), precision=None):
    return lax.dot_general(a, b, (dims, ((), ())), precision=precision, preferred_element_type=F32)


def kernel(
    n_sp,
    n_tp,
    n_dp,
    heads,
    condition,
    source,
    gain,
    conv_x,
    conv_b,
    conv_c,
    rate,
    out_gain,
    latent,
    context,
    mod_weight,
    w_x,
    w_b,
    w_c,
    w_dt,
    w_z,
    w_out,
    out,
    lat_all,
    ctx_buf,
    mod_buf,
    wx,
    wb,
    wc,
    wd,
    wz,
    wo,
    acts,
    edges,
    part,
    part_all,
    mods,
    halo,
    hid,
    own,
    fade,
    snd,
    rcv,
    tot,
    snd_o,
    rcv_o,
    local_sem,
    dp_send,
    dp_recv,
    lat_send,
    lat_recv,
    mod1_send,
    mod1_recv,
    mod2_send,
    mod2_recv,
    edge_send,
    edge_recv,
    chain_send,
    chain_recv,
    t_send,
    t_recv,
    o_send,
    o_recv,
):
    s = lax.axis_index("sp")
    t = lax.axis_index("tp")
    d = lax.axis_index("dp")
    own_rows, width = latent.shape
    ctx_rows = context.shape[0]
    depth = mod_weight.shape[1]
    rows = n_tp * own_rows
    inner = w_x.shape[1]
    both = 2 * inner
    head_dim = inner // heads
    nh2 = 2 * heads

    def remote(src, dst, send, recv, **to):
        return pltpu.make_async_remote_copy(
            src_ref=src, dst_ref=dst, send_sem=send, recv_sem=recv, device_id=to, device_id_type=MESH
        )

    up, down = lax.rem(s + 1, n_sp), lax.rem(s + n_sp - 1, n_sp)
    barrier = pltpu.get_barrier_semaphore()

    def greet(**to):
        pl.semaphore_signal(barrier, inc=1, device_id=to, device_id_type=MESH)

    for k in range(1, n_sp):
        greet(sp=lax.rem(s + k, n_sp))
    for k in range(1, n_tp):
        beside = lax.rem(t + k, n_tp)
        greet(tp=beside)
        greet(sp=up, tp=beside)
        greet(sp=down, tp=beside)
    for k in range(1, n_dp):
        greet(dp=lax.rem(d + k, n_dp))

    local = []

    def fetch(src, dst):
        copy = pltpu.make_async_copy(src, dst, local_sem.at[len(local)])
        copy.start()
        local.append(copy)
        return copy

    mod_copy = fetch(mod_weight, mod_buf)
    lat_copy = fetch(latent, lat_all.at[t])
    ctx_copy = fetch(context, ctx_buf)
    lat_moves = []
    for k in range(1, n_tp):
        lat_moves.append(
            remote(latent, lat_all.at[t], lat_send.at[k], lat_recv.at[k], tp=lax.rem(t + k, n_tp))
        )
    weight_moves = []
    pairs = ((w_x, wx), (w_b, wb), (w_dt, wd), (w_c, wc), (w_z, wz), (w_out, wo))
    for i, (src, dst) in enumerate(pairs):
        count = src.shape[0]
        place = dst.at[d] if src is w_dt else dst.at[pl.ds(d * count, count)]
        for k in range(1, n_dp):
            at = i * n_dp + k
            weight_moves.append(
                remote(src, place, dp_send.at[at], dp_recv.at[at], dp=lax.rem(d + k, n_dp))
            )
        fetch(src, place)

    active = silu(jnp.concatenate([condition[...].astype(F32), row_of(source)], axis=0))
    for j in range(n_sp):
        acts[j, 0:2] = active[:, j * depth : (j + 1) * depth]
    own_acts = jnp.concatenate([acts[s, 0:2], jnp.zeros((PAD - 2, depth), F32)], axis=0).astype(BF16)
    mod_copy.wait()
    pieces = [dot(own_acts, mod_buf[k])[0:2] for k in range(mod_buf.shape[0])]
    cols = pieces[0].shape[1]
    part[...] = jnp.concatenate(pieces + [jnp.zeros((2, cols), F32)], axis=0)
    pl.semaphore_wait(barrier, n_sp + 3 * n_tp + n_dp - 5)
    moves = []
    for k in range(1, n_sp):
        moves.append(
            remote(part, part_all.at[k], mod1_send.at[k], mod1_recv.at[k], sp=lax.rem(s + k, n_sp))
        )
        moves[-1].start()
    for copy in lat_moves + weight_moves:
        copy.start()
    lat_copy.wait()
    edges[0] = lat_all[t, 0:1].astype(F32)
    edges[1] = lat_all[t, own_rows - 1 : own_rows].astype(F32)
    ctx_copy.wait()
    edges[2] = ctx_buf[0:1].astype(F32)
    edges[3] = ctx_buf[ctx_rows - 1 : ctx_rows].astype(F32)
    ctx_up = remote(edges.at[3], halo.at[2], edge_send.at[0], edge_recv.at[2], sp=up)
    ctx_down = remote(edges.at[2], halo.at[3], edge_send.at[1], edge_recv.at[3], sp=down)
    ctx_up.start()
    ctx_down.start()
    lat_up = [
        remote(edges.at[1], halo.at[0], edge_send.at[2 + u], edge_recv.at[0], sp=up, tp=u)
        for u in range(n_tp)
    ]
    lat_down = [
        remote(edges.at[0], halo.at[1], edge_send.at[2 + n_tp + u], edge_recv.at[1], sp=down, tp=u)
        for u in range(n_tp)
    ]

    @pl.when(t == n_tp - 1)
    def _():
        for copy in lat_up:
            copy.start()

    @pl.when(t == 0)
    def _():
        for copy in lat_down:
            copy.start()

    summed = part[...]
    for k in range(1, n_sp):
        moves[k - 1].wait()
        summed = summed + part_all[k]
    mods[t] = summed
    moves = []
    for k in range(1, n_tp):
        moves.append(
            remote(mods.at[t], mods.at[t], mod2_send.at[k], mod2_recv.at[k], tp=lax.rem(t + k, n_tp))
        )
        moves[-1].start()
    for copy in moves:
        copy.wait()

    def vector(row):
        return jnp.concatenate([mods[c][row : row + 1] for c in range(n_tp)], axis=1)

    def normed(v, gains, shift):
        return v * lax.rsqrt(jnp.mean(v * v, axis=1, keepdims=True) + EPSILON) * gains + shift

    gain_row = row_of(gain)
    lat_shift, ctx_shift = vector(0), vector(1)
    lat_gain = gain_row * (1.0 + vector(2))
    ctx_gain = gain_row * (1.0 + vector(3))
    step_rows = min(32, ctx_rows)
    for r in range(0, ctx_rows, step_rows):
        block = ctx_buf[r : r + step_rows].astype(F32)
        hid[rows + PAD + r : rows + PAD + r + step_rows] = normed(block, ctx_gain, ctx_shift).astype(BF16)
    for copy in lat_moves:
        copy.wait()
    for u in range(n_tp):
        hid[u * own_rows : (u + 1) * own_rows] = normed(
            lat_all[u].astype(F32), lat_gain, lat_shift
        ).astype(BF16)
    ctx_up.wait_send()
    ctx_down.wait_send()
    ctx_up.wait_recv()
    ctx_down.wait_recv()
    lat_up[0].wait_recv()
    lat_down[0].wait_recv()

    @pl.when(t == n_tp - 1)
    def _():
        for copy in lat_up:
            copy.wait_send()

    @pl.when(t == 0)
    def _():
        for copy in lat_down:
            copy.wait_send()

    hid[rows : rows + PAD] = jnp.concatenate(
        [
            normed(halo[0], lat_gain, lat_shift),
            normed(halo[1], lat_gain, lat_shift),
            normed(halo[2], ctx_gain, ctx_shift),
            normed(halo[3], ctx_gain, ctx_shift),
            jnp.zeros((PAD - 4, width), F32),
        ],
        axis=0,
    ).astype(BF16)
    for copy in weight_moves:
        copy.wait()
    for copy in local[3:]:
        copy.wait()

    has_before = s > 0
    has_after = s < n_sp - 1

    def shaped(values, before, after, taps):
        count = values.shape[0]
        at = lax.broadcasted_iota(jnp.int32, values.shape, 0)
        before = jnp.where(has_before, before, 0.0)
        after = jnp.where(has_after, after, 0.0)
        earlier = jnp.where(at == 0, before, pltpu.roll(values, 1, 0))
        later = jnp.where(at == count - 1, after, pltpu.roll(values, count - 1, 0))
        w = taps[...].astype(F32)
        return silu(earlier * w[0:1] + values * w[1:2] + later * w[2:3]).astype(BF16)

    def project(weight, count):
        return dot(hid[0:count], weight[...]).astype(BF16).astype(F32)

    total = rows + PAD + ctx_rows
    features = None
    half = wd.shape[3]
    for r in range(n_dp):
        taps = jnp.concatenate(
            [wd[r, 0].astype(F32), wd[r, 1].astype(F32), jnp.zeros((LANES - nh2, half), F32)], axis=0
        ).astype(BF16)
        one = dot(hid[0:total, r * half : (r + 1) * half], taps, ((1,), (1,)))
        features = one if features is None else features + one
    step_all = softplus(features.astype(BF16).astype(F32))
    rates = jnp.concatenate([rate[0:1], rate[1:2], jnp.zeros((1, LANES - nh2), F32)], axis=1)


    def running(steps):
        count = steps.shape[0]
        logs = -rates * steps
        a = lax.broadcasted_iota(jnp.int32, (count, count), 0)
        b = lax.broadcasted_iota(jnp.int32, (count, count), 1)
        lower = jnp.where(a >= b, 1.0, 0.0)
        upper = jnp.where(a <= b, 1.0, 0.0)
        lane = lax.broadcasted_iota(jnp.int32, logs.shape, 1)
        sums = jnp.where(
            lane < heads,
            dot(lower, logs, precision=lax.Precision.HIGHEST),
            dot(upper, logs, precision=lax.Precision.HIGHEST),
        )
        row_lane = lax.broadcasted_iota(jnp.int32, (1, LANES), 1)
        ends = jnp.where(row_lane < heads, sums[count - 1 : count], sums[0:1])
        return sums, ends

    c_steps = step_all[rows + PAD :]
    c_sums, c_ends = running(c_steps)
    l_steps = step_all[0:rows]
    l_sums, l_ends = running(l_steps)
    tot[s] = jnp.concatenate([c_ends, l_ends, jnp.zeros((6, LANES), F32)], axis=0)
    t_moves = []
    for k in range(1, n_sp):
        to = lax.rem(s + k, n_sp)
        t_moves.append(remote(tot.at[s], tot.at[s], t_send.at[k], t_recv.at[k], sp=to))
        t_moves[-1].start()

    px = project(wx, total)
    x_in = shaped(px[0:rows], px[rows : rows + 1], px[rows + 1 : rows + 2], conv_x).astype(F32)
    cx_in = shaped(
        px[rows + PAD :], px[rows + 2 : rows + 3], px[rows + 3 : rows + 4], conv_x
    ).astype(F32)
    pb = project(wb, total)
    b_in = shaped(pb[0:rows], pb[rows : rows + 1], pb[rows + 1 : rows + 2], conv_b)
    cb_in = shaped(pb[rows + PAD :], pb[rows + 2 : rows + 3], pb[rows + 3 : rows + 4], conv_b)
    spread_at = lax.broadcasted_iota(jnp.int32, (LANES, both), 0)
    spread_to = lax.broadcasted_iota(jnp.int32, (LANES, both), 1) // head_dim
    spreader = jnp.where((spread_to == spread_at) | (spread_to + nh2 == spread_at), 1.0, 0.0).astype(BF16)

    def expand(v):
        lane = lax.broadcasted_iota(jnp.int32, v.shape, 1)
        high = v.astype(BF16).astype(F32)
        low = pltpu.roll(v - high, nh2, 1)
        packed = jnp.where(lane < nh2, high, jnp.where(lane < 2 * nh2, low, 0.0))
        return dot(packed.astype(BF16), spreader)

    def moved(values, steps):
        wide = jnp.concatenate([values, values], axis=1)
        return (wide * expand(steps)).astype(BF16)

    c_moved = moved(cx_in, c_steps)
    c_scaled = (c_moved.astype(F32) * expand(jnp.exp(c_ends - c_sums))).astype(BF16)
    c_state = dot(cb_in, c_scaled, ((0,), (0,)))
    l_moved = moved(x_in, l_steps)
    l_scaled = (l_moved.astype(F32) * expand(jnp.exp(l_ends - l_sums))).astype(BF16)
    l_state = dot(b_in, l_scaled, ((0,), (0,)))
    pc = project(wc, rows + PAD)
    c_in = shaped(pc[0:rows], pc[rows : rows + 1], pc[rows + 1 : rows + 2], conv_c)
    scores = dot(c_in, b_in, ((1,), (1,)))
    gate = silu(project(wz, rows))
    for copy in t_moves:
        copy.wait()
    row_lane = lax.broadcasted_iota(jnp.int32, (1, LANES), 1)
    c_later = jnp.zeros((1, LANES), F32)
    l_earlier = jnp.zeros((1, LANES), F32)
    for j in range(n_sp):
        left = jnp.where(row_lane < heads, 1, 0) * (s > j).astype(jnp.int32)
        left = left + jnp.where(row_lane < heads, 0, 1) * (s < j).astype(jnp.int32)
        right = jnp.where(row_lane < heads, 1, 0) * (s < j).astype(jnp.int32)
        right = right + jnp.where(row_lane < heads, 0, 1) * (s > j).astype(jnp.int32)
        c_later = c_later + jnp.where(right > 0, tot[j, 0:1], 0.0)
        l_earlier = l_earlier + jnp.where(left > 0, tot[j, 1:2], 0.0)
    fades = expand(
        jnp.exp(
            jnp.concatenate(
                [c_later, l_earlier, l_ends, l_earlier + l_ends, jnp.zeros((4, LANES), F32)], axis=0
            )
        )
    )
    c_state = c_state * fades[0:1]
    l_state = l_state + c_state * fades[3:4]
    cuts = inner // LANES
    for q in range(2):
        for c in range(cuts):
            at = q * inner + c * LANES
            apart = (1 - q) * inner + c * LANES
            own[q, 2 * c] = l_state[:, at : at + LANES]
            own[q, 2 * c + 1] = c_state[:, apart : apart + LANES]
            fade[q, 2 * c, 0:1] = fades[2:3, at : at + LANES]
            fade[q, 2 * c + 1, 0:1] = jnp.ones((1, LANES), F32)

    ends_chain = (s == 0) | (s == n_sp - 1)
    near = jnp.where(2 * s < n_sp, 0, 1)
    far = 1 - near
    messages = 2 * cuts

    def comes(q):
        return jnp.where(q == 0, s, n_sp - 1 - s) > 0

    def goes(q):
        return jnp.where(q == 0, n_sp - 1 - s, s) > 0

    def message(q, m):
        to = jnp.where(q == 0, up, down)
        return remote(snd.at[q, m], rcv.at[q, m], chain_send.at[q, m], chain_recv.at[q, m], sp=to)

    def hop(q, m):
        @pl.when(comes(q))
        def _():
            message(q, m).wait_recv()

        @pl.when(goes(q))
        def _():
            snd[q, m] = (own[q, m] + rcv[q, m].astype(F32) * fade[q, m, 0:1]).astype(BF16)
            message(q, m).start()

    for q in range(2):

        @pl.when(jnp.logical_not(comes(q)))
        def _():
            rcv[q] = jnp.zeros(rcv.shape[1:], BF16)

    @pl.when(ends_chain)
    def _():
        for m in range(messages):
            hop(near, m)

    at_t = lax.broadcasted_iota(jnp.int32, (rows, rows), 0)
    at_s = lax.broadcasted_iota(jnp.int32, (rows, rows), 1)
    sums_t = jnp.transpose(l_sums)

    def weights(lane, keep):
        gap = l_sums[:, lane : lane + 1] - sums_t[lane : lane + 1]
        return jnp.where(keep, scores * jnp.exp(jnp.minimum(gap, 0.0)), 0.0).astype(BF16)

    pair = LANES // head_dim
    inside = []
    lane_head = lax.broadcasted_iota(jnp.int32, (rows, LANES), 1) // head_dim
    for p in range(heads // pair):
        cut = slice(p * LANES, (p + 1) * LANES)
        cut_b = slice(inner + p * LANES, inner + (p + 1) * LANES)
        source = jnp.concatenate([l_moved[:, cut], l_moved[:, cut_b]], axis=0)
        value = None
        for i in range(pair):
            h = p * pair + i
            w = jnp.concatenate([weights(h, at_t >= at_s), weights(heads + h, at_t <= at_s)], axis=1)
            one = dot(w, source)
            value = one if value is None else jnp.where(lane_head == i, one, value)
        inside.append(value)
    inside = jnp.concatenate(inside, axis=1)
    growth = expand(jnp.exp(l_sums))

    lag = messages // 2

    @pl.when(jnp.logical_not(ends_chain))
    def _():
        for m in range(messages + lag):
            if m < messages:
                hop(near, m)
            if m >= lag:
                hop(far, m - lag)

    @pl.when(ends_chain)
    def _():
        for m in range(messages):
            hop(far, m)

    entering = []
    for q in range(2):
        for c in range(cuts):
            at = q * inner + c * LANES
            context_sum = own[1 - q, 2 * c + 1] + rcv[1 - q, 2 * c + 1].astype(F32)
            entering.append(
                (rcv[q, 2 * c].astype(F32) + context_sum * fades[1:2, at : at + LANES]).astype(BF16)
            )
    entering = jnp.concatenate(entering, axis=1)
    carried = dot(c_in, entering) * growth
    gated = (inside + carried[:, 0:inner] + carried[:, inner:both]) * gate
    ny = (
        gated
        * lax.rsqrt(jnp.mean(gated * gated, axis=1, keepdims=True) + EPSILON)
        * row_of(out_gain)
    ).astype(BF16)

    chunks = n_tp
    chunk = width // chunks
    o_moves = []
    for c in range(chunks):
        cut = slice(c * chunk, (c + 1) * chunk)
        result = dot(ny, wo[:, cut]).astype(BF16)
        for u in range(n_tp):
            snd_o[c, u] = result[u * own_rows : (u + 1) * own_rows]
        for k in range(1, n_tp):
            to = lax.rem(t + k, n_tp)
            at = c * n_tp + k
            o_moves.append(remote(snd_o.at[c, to], rcv_o.at[c, k], o_send.at[at], o_recv.at[at], tp=to))
            o_moves[-1].start()
    for q in range(2):

        @pl.when(goes(q))
        def _():
            for m in range(messages):
                message(q, m).wait_send()

    for c in range(chunks):
        mixed = snd_o[c, t].astype(F32)
        for k in range(1, n_tp):
            o_moves[c * (n_tp - 1) + k - 1].wait()
            mixed = mixed + rcv_o[c, k].astype(F32)
        out[:, c * chunk : (c + 1) * chunk] = (mods[c][4:5] * mixed).astype(BF16)


def shards(
    latent,
    condition,
    context,
    context_source,
    mod_weight,
    norm_gain,
    w_x,
    w_b,
    w_c,
    w_z,
    w_dt,
    conv_x,
    conv_b,
    conv_c,
    decay_rate,
    out_gain,
    w_out,
):
    n_sp, n_tp, n_dp = lax.axis_size("sp"), lax.axis_size("tp"), lax.axis_size("dp")
    own_rows, width = latent.shape[1:]
    ctx_rows = context.shape[1]
    depth = mod_weight.shape[1]
    cols = mod_weight.shape[2]
    inner = w_x.shape[1]
    heads = decay_rate.shape[1]
    both = 2 * inner
    rows = n_tp * own_rows
    messages = 2 * (inner // LANES)
    chunk = width // n_tp
    vmem = pl.BlockSpec(memory_space=pltpu.VMEM)
    anywhere = pl.BlockSpec(memory_space=pl.ANY)
    dma = pltpu.SemaphoreType.DMA
    scratch = [
        pltpu.VMEM((n_tp, own_rows, width), BF16),
        pltpu.VMEM((ctx_rows, width), BF16),
        pltpu.VMEM(mod_weight.shape, BF16),
        pltpu.VMEM((w_x.shape[0] * n_dp, inner), BF16),
        pltpu.VMEM((w_b.shape[0] * n_dp, w_b.shape[1]), BF16),
        pltpu.VMEM((w_c.shape[0] * n_dp, w_c.shape[1]), BF16),
        pltpu.VMEM((n_dp, 2, heads, w_dt.shape[1]), BF16),
        pltpu.VMEM((w_z.shape[0] * n_dp, inner), BF16),
        pltpu.VMEM((w_out.shape[0] * n_dp, width), BF16),
        pltpu.VMEM((n_sp, 8, depth), F32),
        pltpu.VMEM((4, 1, width), F32),
        pltpu.VMEM((8, cols), F32),
        pltpu.VMEM((n_sp, 8, cols), F32),
        pltpu.VMEM((n_tp, 8, cols), F32),
        pltpu.VMEM((4, 1, width), F32),
        pltpu.VMEM((rows + PAD + ctx_rows, width), BF16),
        pltpu.VMEM((2, messages, STATE, LANES), F32),
        pltpu.VMEM((2, messages, 8, LANES), F32),
        pltpu.VMEM((2, messages, STATE, LANES), BF16),
        pltpu.VMEM((2, messages, STATE, LANES), BF16),
        pltpu.VMEM((n_sp, 8, LANES), F32),
        pltpu.VMEM((n_tp, n_tp, own_rows, chunk), BF16),
        pltpu.VMEM((n_tp, n_tp, own_rows, chunk), BF16),
        dma((9,)),
        dma((6 * n_dp,)),
        dma((6 * n_dp,)),
        dma((n_tp,)),
        dma((n_tp,)),
        dma((n_sp,)),
        dma((n_sp,)),
        dma((n_tp,)),
        dma((n_tp,)),
        dma((2 + 2 * n_tp,)),
        dma((4,)),
        dma((2, messages)),
        dma((2, messages)),
        dma((n_sp,)),
        dma((n_sp,)),
        dma((n_tp * n_tp,)),
        dma((n_tp * n_tp,)),
    ]
    result = pl.pallas_call(
        functools.partial(kernel, n_sp, n_tp, n_dp, heads),
        out_shape=jax.ShapeDtypeStruct((own_rows, width), BF16),
        in_specs=[vmem] * 8 + [anywhere] * 9,
        out_specs=vmem,
        scratch_shapes=scratch,
        compiler_params=pltpu.CompilerParams(
            has_side_effects=True, collective_id=0, vmem_limit_bytes=62_000_000
        ),
    )(
        condition,
        context_source,
        norm_gain,
        conv_x,
        conv_b,
        conv_c,
        decay_rate,
        out_gain,
        latent[0],
        context[0],
        mod_weight,
        w_x,
        w_b,
        w_c,
        jnp.swapaxes(w_dt, 1, 2),
        w_z,
        w_out,
    )
    return result[None]


def solution(mesh):
    placed = (
        P("dp", ("sp", "tp"), None),
        P("dp", None),
        P("dp", "sp", None),
        P(),
        P(None, "sp", "tp"),
        P(),
        P("dp", "tp"),
        P("dp", "tp"),
        P("dp", "tp"),
        P("dp", "tp"),
        P(None, "dp", "tp"),
        P(None, "tp"),
        P(None, "tp"),
        P(None, "tp"),
        P(None, "tp"),
        P("tp"),
        P(("tp", "dp"), None),
    )
    return jax.shard_map(
        shards, mesh=mesh, in_specs=placed, out_specs=P("dp", ("sp", "tp"), None), check_vma=False
    )
```
